256 devices in a mesh: grp: 2 (over y), ep: 32 (over z, core), tp: 4 (over x).
Axes of the slice: x: 4, y: 2, z: 16, core: 2. Of those that a mesh axis runs over, the one named last changes fastest.
The devices are a block of a 4x16x16 slice.
Arguments:
- conv_x: bfloat16 [65536, 2048], P(('grp', 'ep', 'tp')), parts along dimension 0, may hold values from -6 to 6
- conv_c: bfloat16 [65536, 2048], P(('grp', 'ep', 'tp')), parts along dimension 0, may hold values from -6 to 6
- conv_b: bfloat16 [65536, 2048], P(('grp', 'ep', 'tp')), parts along dimension 0, may hold values from -6 to 6
- conv_taps: float32 [3, 2048], replicated, may hold values from -3.5 to 3.5
- w_out: bfloat16 [2048, 2048], P('tp'), may hold values from -0.125 to 0.125
- tokens_b: bfloat16 [32768, 2048], P(('grp', 'ep', 'tp')), parts along dimension 0, may hold values from -6 to 6
- norm_gain: float32 [2048], replicated, may hold values from 0.1 to 1.9
- route_b: int32 [32768, 2], P(('grp', 'ep', 'tp')), parts along dimension 0, may hold values from 0 to 31, all different within a row; in each aligned block of 128 rows (0 to 127, 128 to 255, ...) at most 16 rows name the same one
- route_weights: float32 [32768, 2], P(('grp', 'ep', 'tp')), parts along dimension 0, may hold values from 0.1 to 1
- w_gate: bfloat16 [32, 2048, 1024], P('ep', None, 'tp'), may hold values from -0.125 to 0.125
- w_up: bfloat16 [32, 2048, 1024], P('ep', None, 'tp'), may hold values from -0.125 to 0.125
- w_down: bfloat16 [32, 1024, 2048], P('ep', 'tp'), may hold values from -0.1875 to 0.1875
Outputs:
- mixed_a: bfloat16 [65536, 2048], P(('grp', 'ep', 'tp')), parts along dimension 0
- experts_b: bfloat16 [32768, 2048], P(('grp', 'ep', 'tp')), parts along dimension 0
The draws below stay inside these ranges and needn't reach their ends.
There are 2 independent parts, one for each index of `grp`. The reference program is written for one: setup_inputs(seed, part) draws one part's arguments, and reference() takes and returns one part's arrays. A program takes and returns all parts, laid end to end along the dimension named above; an argument that names none is the same for every part. Nothing has to cross between parts.
Inputs may be any that keep to these rules, and one draw needn't show every extreme that they name: `route_b`: the 2 experts of a row differ. Within the 128 rows of one device no expert is named more than 16 times, and in every draw some device names some expert exactly 16 times.
All inputs are finite; a program needn't handle non-finite values.
Results may differ from the reference program's by a relative error of at most 0.012.
Values may be sent and summed in bfloat16 or wider, within the bound.
A program may use at most 128 MiB of HBM per device.

```python
import math
import jax
import jax.numpy as jnp
import numpy as np
from jax import lax

D = 2048
CH = 2048
CONV = 3
FF = 1024
TOPK = 2
ROWS_B = 128
EXPERTS = 32
CAP = 16
SEQ = 32768
TOKENS_B = 16384
N_EP = 32
N_TP = 4


def steps_of(stream_key, shape, cuts, low, high):
    factor_of = 1.0
    for axis_at, blocks in cuts:
        draws = jax.random.uniform(jax.random.fold_in(jax.random.fold_in(stream_key, 6), axis_at), (blocks,), jnp.float32, low / len(cuts), high / len(cuts))
        factor_of = factor_of * jnp.repeat(jnp.exp(draws), shape[axis_at] // blocks).reshape((-1,) + (1,) * (len(shape) - 1 - axis_at))
    return factor_of


def assign_block(stream_key, own, number, rows, count, top, bound, slope):
    sequence = jax.random.permutation(stream_key, count)
    heavy_load, usual = portions_of(count, rows * top, bound, slope, True), portions_of(count, rows * top, bound, slope, False)
    places = jnp.arange(count)

    def named(tallies, offset_by):
        used = int((tallies > 0).sum())
        fixed = max(1, used // 4)
        shifted = fixed + (places - fixed + offset_by * (used - fixed)) % max(1, count - fixed)
        return jnp.zeros((count,), jnp.int32).at[sequence[jnp.where(places < fixed, places, shifted)]].set(jnp.asarray(tallies, jnp.int32))

    tallies = jnp.where(number % 4 == 0, named(heavy_load, number // 4), named(usual, number - number // 4 - 1))
    mixed = jax.random.permutation(jax.random.fold_in(own, 3), count)
    giver, sink = mixed[0:count // 2 * 2:2], mixed[1:count // 2 * 2:2]
    slack = jnp.minimum(tallies[giver] - 1, bound - tallies[sink]) // 2
    slack = jnp.where((giver == sequence[0]) | (sink == sequence[0]) | (tallies[sink] == 0), 0, jnp.maximum(slack, 0))
    shifted = jax.random.randint(jax.random.fold_in(own, 4), (count // 2,), 0, 1 << 20) % (slack + 1)
    tallies = tallies.at[giver].add(-shifted).at[sink].add(shifted)
    members = jnp.searchsorted(jnp.cumsum(tallies), jnp.arange(rows * top), side="right").astype(jnp.int32)
    table = members.reshape(top, rows).T
    table = table[jax.random.permutation(jax.random.fold_in(own, 1), rows)]
    offset_by = jax.random.randint(jax.random.fold_in(own, 2), (rows, 1), 0, top)
    return jnp.take_along_axis(table, (jnp.arange(top)[None, :] + offset_by) % top, axis=1)


def portions_of(count, total, most, lean, full):
    weights = [(1 << 20) // math.isqrt(standing ** lean) + 1 for standing in range(1, count + 1)]
    largest = most if full else min(most, max(-(-total // count), total * weights[0] // sum(weights)))
    least = 1 if total - largest >= count - 1 else 0
    counts, rest = [largest] + [least] * (count - 1), total - largest - least * (count - 1)
    while rest > 0:
        candidates = [i for i in range(1, count) if counts[i] < largest] or [i for i in range(1, count) if counts[i] < most]
        mass, left = sum([weights[i] for i in candidates]), rest
        for i in candidates:
            addition = min(most - counts[i], max(1, left * weights[i] // mass), rest)
            counts[i] = counts[i] + addition
            rest = rest - addition
    return np.array(counts)


def bell_draw(key, dims, spread, most, cuts=(), kind=jnp.bfloat16):
    entries = spread * jax.random.normal(key, dims, jnp.float32)
    if cuts:
        entries = entries * steps_of(key, dims, cuts, -0.22, 0.18)
    return jnp.clip(entries, -most, most).astype(kind)


def setup_inputs(seed: int = 0, part: int = 0) -> dict:
    streams_of = jax.random.split(jax.random.key(seed), 13)
    own_keys = jax.random.split(jax.random.fold_in(streams_of[12], part), 13)
    conv_x = bell_draw(own_keys[0], (SEQ, CH), 1.0, 6.0, ((0, 128),))
    conv_c = bell_draw(own_keys[1], (SEQ, CH), 1.0, 6.0, ((0, 128),))
    conv_b = bell_draw(own_keys[2], (SEQ, CH), 1.0, 6.0, ((0, 128),))
    conv_taps = bell_draw(streams_of[3], (CONV, CH), CONV ** -0.5, 3.5, (), jnp.float32)
    w_out = bell_draw(streams_of[4], (CH, D), CH ** -0.5, 0.125, ((0, 4),))
    tokens_b = bell_draw(own_keys[5], (TOKENS_B, D), 1.0, 6.0, ((0, 128),))
    norm_gain = jnp.clip(1.0 + 0.18 * jax.random.normal(streams_of[6], (D,), jnp.float32), 0.1, 1.9)
    route_b_keys = jax.random.split(jax.random.fold_in(own_keys[7], 1), TOKENS_B // ROWS_B)
    route_b_turns = jax.random.permutation(jax.random.fold_in(own_keys[7], 3), TOKENS_B // ROWS_B)
    route_b = jax.vmap(lambda own, number: assign_block(jax.random.fold_in(own_keys[7], 2), own, number, ROWS_B, EXPERTS, TOPK, CAP, 2))(route_b_keys, route_b_turns).reshape((TOKENS_B, TOPK))
    route_weights = jnp.clip(jnp.exp(math.log(1.0) - 2.3025851 * jax.random.uniform(own_keys[8], (TOKENS_B, TOPK), jnp.float32) ** steps_of(own_keys[8], (TOKENS_B, TOPK), ((0, 128),), -0.2, 0.2)), 0.1, 1.0)
    w_gate = bell_draw(streams_of[9], (EXPERTS, D, FF), D ** -0.5, 0.125, ((0, 32), (2, 4)))
    w_up = bell_draw(streams_of[10], (EXPERTS, D, FF), D ** -0.5, 0.125, ((0, 32), (2, 4)))
    w_down = bell_draw(streams_of[11], (EXPERTS, FF, D), FF ** -0.5, 0.1875, ((0, 32), (1, 4)))
    return {"conv_x": conv_x, "conv_c": conv_c, "conv_b": conv_b, "conv_taps": conv_taps, "w_out": w_out, "tokens_b": tokens_b, "norm_gain": norm_gain, "route_b": route_b, "route_weights": route_weights, "w_gate": w_gate, "w_up": w_up, "w_down": w_down}


def slot_ranks(route):
    flat = route.reshape(-1)
    onehot = (flat[:, None] == jnp.arange(EXPERTS, dtype=jnp.int32)[None, :]).astype(jnp.int32)
    earlier = jnp.cumsum(onehot, axis=0) - onehot
    return lax.optimization_barrier(jnp.sum(earlier * onehot, axis=1)).reshape(route.shape)

def reference(conv_x, conv_c, conv_b, conv_taps, w_out, tokens_b, norm_gain, route_b, route_weights, w_gate, w_up, w_down):
    mixed_u = (conv_c.astype(jnp.float32) * conv_x.astype(jnp.float32)).astype(jnp.bfloat16)
    extended = jnp.concatenate([jnp.zeros((CONV - 1, CH), jnp.bfloat16), mixed_u], axis=0)
    filtered = jnp.zeros((SEQ, CH), jnp.float32)
    for shift_tap in range(CONV):
        filtered = filtered + conv_taps[shift_tap][None, :] * extended[shift_tap:shift_tap + SEQ].astype(jnp.float32)
    gated = (conv_b.astype(jnp.float32) * filtered).astype(jnp.bfloat16)
    mixed_a = jnp.dot(gated, w_out, preferred_element_type=jnp.float32).astype(jnp.bfloat16)
    tokens_f = tokens_b.astype(jnp.float32)
    normed = (tokens_f * lax.rsqrt(lax.optimization_barrier(jnp.mean(tokens_f * tokens_f, axis=-1, keepdims=True)) + 1e-06) * norm_gain).astype(jnp.bfloat16)
    sources = N_EP * N_TP
    slots = jax.vmap(slot_ranks)(route_b.reshape(sources, ROWS_B, TOPK)).reshape(TOKENS_B, TOPK)
    source_id = (jnp.arange(TOKENS_B, dtype=jnp.int32) // ROWS_B)[:, None]
    position = source_id * CAP + slots
    token_id = jnp.broadcast_to(jnp.arange(TOKENS_B, dtype=jnp.int32)[:, None], (TOKENS_B, TOPK))
    fill_table = jnp.full((EXPERTS, sources * CAP), TOKENS_B, jnp.int32)
    fill_table = fill_table.at[route_b.reshape(-1), position.reshape(-1)].set(token_id.reshape(-1))
    padded = jnp.concatenate([normed, jnp.zeros((1, D), jnp.bfloat16)], axis=0)

    def one_expert(operands):
        fill_row, gate_w, up_w, down_w = operands
        rows = padded[fill_row]
        gate_val = jnp.dot(rows, gate_w, preferred_element_type=jnp.float32)
        up_val = jnp.dot(rows, up_w, preferred_element_type=jnp.float32)
        hidden = (jax.nn.silu(gate_val) * up_val).astype(jnp.bfloat16)
        blocks = hidden.reshape(-1, N_TP, FF // N_TP).astype(jnp.float32)
        down_blocks = down_w.reshape(N_TP, FF // N_TP, D).astype(jnp.float32)
        partial_sums = jnp.einsum('rqf,qfd->qrd', blocks, down_blocks).astype(jnp.bfloat16)
        partial_sums = lax.optimization_barrier(partial_sums)
        return lax.optimization_barrier(jnp.sum(partial_sums.astype(jnp.float32), axis=0)).astype(jnp.bfloat16)
    results = lax.map(one_expert, (fill_table, w_gate, w_up, w_down))
    flat_results = results.reshape(EXPERTS * sources * CAP, D)
    picked = flat_results[route_b * (sources * CAP) + position]
    shares = route_weights / lax.optimization_barrier(jnp.sum(route_weights, axis=-1, keepdims=True))
    experts_b = lax.optimization_barrier(jnp.sum(picked.astype(jnp.float32) * shares[:, :, None], axis=1)).astype(jnp.bfloat16)
    return (mixed_a, experts_b)
```

```python
import jax
import jax.numpy as jnp
from jax import lax
from jax.sharding import PartitionSpec as P

D = 2048
TOPK = 2


def shifted(x, axis, by):
    size = lax.axis_size(axis)
    pairs = [(i, i + by) for i in range(size) if 0 <= i + by < size]
    return lax.ppermute(x, axis, pairs)


def slot_targets(route, experts, capacity):
    flat = route.reshape(-1)
    onehot = (flat[:, None] == jnp.arange(experts, dtype=jnp.int32)[None, :]).astype(jnp.int32)
    earlier = jnp.cumsum(onehot, axis=0) - onehot
    ranks = jnp.sum(earlier * onehot, axis=1).reshape(route.shape)
    return route * capacity + ranks


def fill_slots(targets, slot_total, filler):
    token_ids = jnp.repeat(jnp.arange(filler, dtype=jnp.int32), targets.shape[1])
    return jnp.full((slot_total,), filler, jnp.int32).at[targets.reshape(-1)].set(token_ids)


def expert_hidden(rows, weight_gate, weight_up):
    gate_val = jnp.dot(rows, weight_gate, preferred_element_type=jnp.float32)
    up_val = jnp.dot(rows, weight_up, preferred_element_type=jnp.float32)
    return (jax.nn.silu(gate_val) * up_val).astype(jnp.bfloat16)


def per_device(
    conv_x,
    conv_c,
    conv_b,
    conv_taps,
    w_out,
    tokens_b,
    norm_gain,
    route_b,
    route_weights,
    w_gate,
    w_up,
    w_down,
):
    rows_mix = conv_x.shape[0]
    reach_rows = conv_taps.shape[0] - 1
    mixed_u = (conv_c.astype(jnp.float32) * conv_x.astype(jnp.float32)).astype(jnp.bfloat16)
    before = shifted(mixed_u[rows_mix - reach_rows :], ("ep", "tp"), 1)
    extended = jnp.concatenate([before, mixed_u], axis=0)
    filtered = jnp.zeros(mixed_u.shape, jnp.float32)
    for shift_tap in range(reach_rows + 1):
        filtered = filtered + conv_taps[shift_tap][None, :] * extended[
            shift_tap : shift_tap + rows_mix
        ].astype(jnp.float32)
    gated_rows = (conv_b.astype(jnp.float32) * filtered).astype(jnp.bfloat16)
    mixed_out = jnp.dot(
        gated_rows,
        lax.all_gather(w_out, "tp", axis=0, tiled=True),
        preferred_element_type=jnp.float32,
    )
    mixed_a = mixed_out.astype(jnp.bfloat16)
    tokens_f = tokens_b.astype(jnp.float32)
    normed = (
        tokens_f
        * lax.rsqrt(jnp.mean(tokens_f * tokens_f, axis=-1, keepdims=True) + 1e-06)
        * norm_gain
    ).astype(jnp.bfloat16)
    experts = lax.axis_size("ep")
    rows_exp = route_b.shape[0]
    capacity = 2 * rows_exp * TOPK // experts
    slot_total = experts * capacity
    targets = slot_targets(route_b, experts, capacity)
    weight_gate = lax.all_gather(w_gate[0], "tp", axis=0, tiled=False)
    weight_up = lax.all_gather(w_up[0], "tp", axis=0, tiled=False)
    weight_down = lax.all_gather(w_down[0], "tp", axis=0, tiled=False)
    padded_rows = jnp.concatenate([normed, jnp.zeros((1, D), jnp.bfloat16)], axis=0)
    outgoing = padded_rows[fill_slots(targets, slot_total, rows_exp)]
    arrived = lax.all_to_all(outgoing, "ep", split_axis=0, concat_axis=0, tiled=True)
    summed = jnp.zeros(arrived.shape, jnp.float32)
    for block in range(lax.axis_size("tp")):
        hidden = expert_hidden(arrived, weight_gate[block], weight_up[block])
        summed = summed + jnp.dot(hidden, weight_down[block], preferred_element_type=jnp.float32)
    summed = summed.astype(jnp.bfloat16)
    returned = lax.all_to_all(summed, "ep", split_axis=0, concat_axis=0, tiled=True)
    picked = returned[targets]
    shares = route_weights / jnp.sum(route_weights, axis=-1, keepdims=True)
    experts_b = jnp.sum(picked.astype(jnp.float32) * shares[:, :, None], axis=1).astype(
        jnp.bfloat16
    )
    return (mixed_a, experts_b)


def solution(mesh):
    return jax.shard_map(
        per_device,
        mesh=mesh,
        in_specs=(
            P(("grp", "ep", "tp"), None),
            P(("grp", "ep", "tp"), None),
            P(("grp", "ep", "tp"), None),
            P(),
            P("tp", None),
            P(("grp", "ep", "tp"), None),
            P(),
            P(("grp", "ep", "tp"), None),
            P(("grp", "ep", "tp"), None),
            P("ep", None, "tp"),
            P("ep", None, "tp"),
            P("ep", "tp", None),
        ),
        out_specs=(P(("grp", "ep", "tp"), None), P(("grp", "ep", "tp"), None)),
        check_vma=False,
    )
```

```python
import functools
import jax
import jax.numpy as jnp
from jax import lax
from jax.experimental import pallas as pl
from jax.experimental.pallas import tpu as pltpu
from jax.sharding import PartitionSpec as P

TOPK = 2
CORES = 2
LANES = 128
META_ROWS = 8
MESH = pl.DeviceIdType.MESH
BF16 = jnp.bfloat16
F32 = jnp.float32


def fused(
    n_ep,
    n_tp,
    cap,
    tokens,
    meta,
    gain,
    wg,
    wu,
    wd,
    wo,
    cx,
    cc,
    cb,
    taps,
    mix_out,
    exp_out,
    tok,
    meta_buf,
    gbuf,
    ubuf,
    dbuf,
    obuf,
    rows,
    wslot,
    hid,
    rcat,
    rout,
    acc,
    pt,
    conv,
    uext,
    gated,
    halo_out,
    halo_in,
    lsem,
    xs,
    xr,
    zs,
    zr,
    ps,
    pr,
    ms,
    mr,
    pms,
    pmr,
    qs,
    qr,
    rs,
    rr,
    hs,
    hr,
):
    nz = n_ep // CORES
    far = nz // 2
    ep = lax.axis_index("ep")
    tp = lax.axis_index("tp")
    z = ep // CORES
    core = ep % CORES
    n_rows = tokens.shape[0]
    d_model = tokens.shape[1]
    half = n_rows // 2

    tp_at = [{"tp": (tp + 1) % n_tp}, {"tp": (tp + n_tp - 1) % n_tp}]
    z_at = [
        {"ep": ((z + 1) % nz) * CORES + core},
        {"ep": ((z + nz - 1) % nz) * CORES + core},
    ]
    partner = {"ep": z * CORES + (1 - core)}
    lin = ep * n_tp + tp
    total = n_ep * n_tp
    after = (lin + 1) % total
    prior = (lin + total - 1) % total
    after_at = {"ep": after // n_tp, "tp": after % n_tp}
    prior_at = {"ep": prior // n_tp, "tp": prior % n_tp}

    barrier = pltpu.get_barrier_semaphore()
    peers = tp_at + z_at + [partner, after_at, prior_at]
    for peer in peers:
        pl.semaphore_signal(barrier, inc=1, device_id=peer, device_id_type=MESH)

    local = [
        pltpu.make_async_copy(tokens, tok.at[0, z], lsem.at[0]),
        pltpu.make_async_copy(meta, meta_buf.at[0, z], lsem.at[1]),
        pltpu.make_async_copy(wg.at[0], gbuf.at[tp], lsem.at[2]),
        pltpu.make_async_copy(wu.at[0], ubuf.at[tp], lsem.at[3]),
        pltpu.make_async_copy(wd.at[0], dbuf.at[tp], lsem.at[4]),
        pltpu.make_async_copy(wo, obuf.at[tp], lsem.at[5]),
        pltpu.make_async_copy(cx, conv.at[0], lsem.at[6]),
        pltpu.make_async_copy(cc, conv.at[1], lsem.at[7]),
        pltpu.make_async_copy(cb, conv.at[2], lsem.at[8]),
    ]
    for copy in local:
        copy.start()

    blocks = [(wg.at[0], gbuf), (wu.at[0], ubuf), (wd.at[0], dbuf), (wo, obuf)]

    def x_send(a, d, hop):
        src, buf = blocks[a]
        if hop == 0:
            dst = buf.at[tp]
        else:
            owner = (tp + n_tp - 1) % n_tp if d == 0 else (tp + 1) % n_tp
            part = buf.shape[1] // 2
            dst = buf.at[owner, pl.ds(d * part, part)]
            src = dst
        return pltpu.make_async_remote_copy(
            src_ref=src,
            dst_ref=dst,
            send_sem=xs.at[a, d, hop],
            recv_sem=xr.at[a, d, hop],
            device_id=tp_at[d],
            device_id_type=MESH,
        )

    def x_wait(a, d, hop):
        x_send(a, d, hop).wait_recv()

    def x_forward(a):
        for d in (0, 1):
            x_wait(a, d, 0)
            x_send(a, d, 1).start()

    def away(d, h):
        return (z + (nz - h if d == 0 else h)) % nz

    def z_send(d, h, ch):
        ref = tok.at[0, away(d, h - 1), pl.ds(ch * half, half)]
        return pltpu.make_async_remote_copy(
            src_ref=ref,
            dst_ref=ref,
            send_sem=zs.at[d, h - 1, ch],
            recv_sem=zr.at[d, h - 1, ch],
            device_id=z_at[d],
            device_id_type=MESH,
        )

    def m_send(d, h):
        ref = meta_buf.at[0, away(d, h - 1)]
        return pltpu.make_async_remote_copy(
            src_ref=ref,
            dst_ref=ref,
            send_sem=ms.at[d, h - 1],
            recv_sem=mr.at[d, h - 1],
            device_id=z_at[d],
            device_id_type=MESH,
        )

    def p_send(d, h, ch):
        at = (away(d, h), pl.ds(ch * half, half))
        return pltpu.make_async_remote_copy(
            src_ref=tok.at[(0,) + at],
            dst_ref=tok.at[(1,) + at],
            send_sem=ps.at[d, h, ch],
            recv_sem=pr.at[d, h, ch],
            device_id=partner,
            device_id_type=MESH,
        )

    def pm_send(d, h):
        at = away(d, h)
        return pltpu.make_async_remote_copy(
            src_ref=meta_buf.at[0, at],
            dst_ref=meta_buf.at[1, at],
            send_sem=pms.at[d, h],
            recv_sem=pmr.at[d, h],
            device_id=partner,
            device_id_type=MESH,
        )

    def held(d, h):
        if h == 0:
            return (0, 1) if d == 0 else ()
        return (0, 1) if h < far else (d,)

    def meta_held(d, h):
        return 0 < h < far or d == 0

    halo = pltpu.make_async_remote_copy(
        src_ref=halo_out,
        dst_ref=halo_in,
        send_sem=hs.at[0],
        recv_sem=hr.at[0],
        device_id=after_at,
        device_id_type=MESH,
    )

    tri = (
        lax.broadcasted_iota(jnp.int32, (LANES, LANES), 0)
        < lax.broadcasted_iota(jnp.int32, (LANES, LANES), 1)
    ).astype(F32).astype(BF16)

    def select(rel, zz):
        info = meta_buf[rel, zz]
        first, second = info[0:1], info[1:2]
        mine = ep.astype(F32)
        other = (z * CORES + (1 - core)).astype(F32)
        one = jnp.ones((1, LANES), F32)
        none = jnp.zeros((1, LANES), F32)
        hit = jnp.where(first == mine, one, jnp.where(second == mine, one, none))
        hit_p = jnp.where(first == other, one, jnp.where(second == other, one, none))
        share = jnp.where(
            first == mine, info[2:3], jnp.where(second == mine, info[3:4], none)
        )
        at_row = lax.broadcasted_iota(jnp.int32, (META_ROWS, LANES), 0)
        both = jnp.where(at_row == 0, hit, jnp.where(at_row == 1, hit_p, 0.0))
        rank = jnp.dot(both.astype(BF16), tri, preferred_element_type=F32)
        place = jnp.where(hit > 0, rank[0:1], -1.0)
        place_p = jnp.where(hit_p > 0, rank[1:2] + float(cap), -1.0)
        slot = lax.broadcasted_iota(jnp.int32, (LANES, LANES), 0).astype(F32)
        pick = jnp.where(slot[:cap] == place, 1.0, 0.0)
        base = pl.multiple_of((rel * nz + zz) * cap, cap)
        got = jnp.dot(pick.astype(BF16), tok[rel, zz], preferred_element_type=F32)
        mean = jnp.mean(got * got, axis=-1, keepdims=True)
        normed = got * lax.rsqrt(mean + 1e-06) * gain[...]
        rows[pl.ds(base, cap), :] = normed.astype(BF16)
        weight = jnp.sum(pick * share, axis=-1, keepdims=True)
        wslot[pl.ds(base, cap), :] = jnp.broadcast_to(weight, (cap, LANES))
        spread = jnp.where(slot == place, 1.0, jnp.where(slot == place_p, 1.0, 0.0))
        return spread

    def select_own(zz):
        pt[zz] = jnp.transpose(select(0, zz)).astype(BF16)

    def select_partner(zz):
        select(1, zz)

    local[6].wait()
    local[7].wait()
    tail = halo_out.shape[0]
    last = conv.shape[1] - tail
    halo_out[...] = (
        conv[0, pl.ds(last, tail), :].astype(F32) * conv[1, pl.ds(last, tail), :].astype(F32)
    ).astype(BF16)
    local[0].wait()
    local[1].wait()
    pl.semaphore_wait(barrier, len(peers))

    for a in (0, 1, 2):
        for d in (0, 1):
            x_send(a, d, 0).start()
    for d in (0, 1):
        m_send(d, 1).start()
    for ch in (0, 1):
        for d in (0, 1):
            z_send(d, 1, ch).start()
    halo.start()
    pm_send(0, 0).start()
    for ch in (0, 1):
        p_send(0, 0, ch).start()

    local[8].wait()
    halo.wait_recv()
    n_conv = conv.shape[1]
    reach = taps.shape[0] - 1
    wide = uext.shape[1]
    edge = jnp.where(lin == 0, 0.0, 1.0)

    @pl.loop(0, d_model // wide)
    def _(n):
        cols = pl.ds(pl.multiple_of(n * wide, wide), wide)
        u = (conv[0, :, cols].astype(F32) * conv[1, :, cols].astype(F32)).astype(BF16)
        uext[pl.ds(tail, n_conv), :] = u.astype(F32)
        uext[pl.ds(0, tail), :] = halo_in[:, cols].astype(F32) * edge
        out = jnp.zeros((n_conv, wide), F32)
        for k in range(reach + 1):
            out = out + taps[pl.ds(k, 1), cols] * uext[pl.ds(tail - reach + k, n_conv), :]
        gated[:, cols] = (conv[2, :, cols].astype(F32) * out).astype(BF16)

    select_own(z)
    pm_send(0, 0).wait_recv()
    for ch in (0, 1):
        p_send(0, 0, ch).wait_recv()
    select_partner(z)

    x_at = {far // 2 - 1: (0,), far // 2 + 1: (1,), far - 1: (2,)} if far > 3 else {far - 1: (0, 1, 2)}
    for h in range(1, far + 1):
        for ch in (0, 1):
            for d in (0, 1):
                if ch in held(d, h):
                    z_send(d, h, ch).wait_recv()
                    if h < far and ch in held(d, h + 1):
                        z_send(d, h + 1, ch).start()
                    p_send(d, h, ch).start()
        for d in (0, 1):
            if meta_held(d, h):
                m_send(d, h).wait_recv()
                if h < far and meta_held(d, h + 1):
                    m_send(d, h + 1).start()
                pm_send(d, h).start()
        for a in x_at.get(h, ()):
            x_forward(a)
        if h == far - 1:
            for d in (0, 1):
                x_send(3, d, 0).start()
        count = 2 if h < far else 1

        @pl.loop(0, count)
        def _(k):
            select_own((z + nz + jnp.where(k == 0, -h, h)) % nz)

        for d in (0, 1):
            if meta_held(d, h):
                pm_send(d, h).wait_recv()
            for ch in held(d, h):
                p_send(d, h, ch).wait_recv()

        @pl.loop(0, count)
        def _(k):
            select_partner((z + nz + jnp.where(k == 0, -h, h)) % nz)

    local[2].wait()
    local[3].wait()
    local[4].wait()

    def hidden(step):
        b = (tp + step) % n_tp
        width = gbuf.shape[2]
        gate_val = jnp.dot(rows[...], gbuf[b], preferred_element_type=F32)
        up_val = jnp.dot(rows[...], ubuf[b], preferred_element_type=F32)
        value = gate_val / (1.0 + jnp.exp(-gate_val)) * up_val
        hid[:, pl.ds(pl.multiple_of(b * width, width), width)] = value.astype(BF16)

    @pl.loop(0, n_tp - 1)
    def _(k):
        hidden(jnp.where(k == 0, 0, jnp.where(k == 1, 1, n_tp - 1)))

    for a in (0, 1):
        for d in (0, 1):
            x_wait(a, d, 1)
    hidden(2)
    for d in (0, 1):
        x_wait(2, d, 1)
    mid = nz * cap
    depth = dbuf.shape[0] * dbuf.shape[1]

    def down(rel, n, width):
        cols = pl.ds(pl.multiple_of(n * width, width), width)
        value = jnp.dot(
            hid[pl.ds(rel * mid, mid), :],
            dbuf[:, :, cols].reshape(depth, width),
            preferred_element_type=F32,
        )
        value = (value * wslot[pl.ds(rel * mid, mid), 0:1]).astype(BF16)
        return cols, value.reshape(nz, cap, width)

    swap = pltpu.make_async_remote_copy(
        src_ref=rout,
        dst_ref=rcat.at[:, pl.ds(cap, cap), :],
        send_sem=qs.at[0],
        recv_sem=qr.at[0],
        device_id=partner,
        device_id_type=MESH,
    )
    out_wide = 512 if d_model % 512 == 0 else d_model

    @pl.loop(0, d_model // out_wide)
    def _(n):
        cols, value = down(1, n, out_wide)
        rout[:, :, cols] = value

    swap.start()

    @pl.loop(0, d_model // out_wide)
    def _(n):
        cols, value = down(0, n, out_wide)
        rcat[:, pl.ds(0, cap), cols] = value

    swap.wait_recv()

    def r_send(d, t, ch):
        at = pl.ds(ch * half, half)
        return pltpu.make_async_remote_copy(
            src_ref=acc.at[d, t - 1, at],
            dst_ref=acc.at[d, t, at],
            send_sem=rs.at[d, t - 1, ch],
            recv_sem=rr.at[d, t - 1, ch],
            device_id=z_at[d],
            device_id_type=MESH,
        )

    def spread_back(zz, ch):
        return jnp.dot(
            pt[zz, pl.ds(ch * half, half), 0 : 2 * cap],
            rcat[zz],
            preferred_element_type=F32,
        )

    def ahead(d, t):
        dist = far + 1 - t
        return (z + dist) % nz if d == 0 else (z + nz - dist) % nz

    def r_step(t, parts):
        for ch, d, arrives in parts:
            at = pl.ds(ch * half, half)
            value = spread_back(ahead(d, t), ch)
            if arrives:
                r_send(d, t - 1, ch).wait_recv()
                value = value + acc[d, t - 1, at].astype(F32)
            acc[d, t - 1, at] = value.astype(BF16)
            r_send(d, t, ch).start()

    r_step(1, [(0, 0, False), (1, 1, False)])
    r_step(2, [(0, 0, True), (1, 1, True), (1, 0, False), (0, 1, False)])
    every = [(0, 0, True), (0, 1, True), (1, 0, True), (1, 1, True)]
    turn = max(3, far - 1)

    @pl.loop(3, turn)
    def _(t):
        r_step(t, every)

    x_forward(3)

    @pl.loop(turn, far + 1)
    def _(t):
        r_step(t, every)

    for ch in (0, 1):
        at = pl.ds(ch * half, half)
        value = spread_back(z, ch)
        for d in (0, 1):
            r_send(d, far, ch).wait_recv()
            value = value + acc[d, far, at].astype(F32)
        exp_out[at, :] = value.astype(BF16)

    local[5].wait()
    for d in (0, 1):
        x_wait(3, d, 1)
    deep = obuf.shape[0] * obuf.shape[1]

    @pl.loop(0, d_model // out_wide)
    def _(n):
        cols = pl.ds(pl.multiple_of(n * out_wide, out_wide), out_wide)
        mix_out[:, cols] = jnp.dot(
            gated[...],
            obuf[:, :, cols].reshape(deep, out_wide),
            preferred_element_type=F32,
        ).astype(BF16)

    for a in range(len(blocks)):
        for d in (0, 1):
            for hop in (0, 1):
                x_send(a, d, hop).wait_send()
    for d in (0, 1):
        for h in range(far + 1):
            if h > 0:
                for ch in held(d, h):
                    z_send(d, h, ch).wait_send()
                if meta_held(d, h):
                    m_send(d, h).wait_send()
            for ch in held(d, h):
                p_send(d, h, ch).wait_send()
            if meta_held(d, h):
                pm_send(d, h).wait_send()
        for t in range(1, far + 1):
            for ch in (d,) if t == 1 else (0, 1):
                r_send(d, t, ch).wait_send()
    swap.wait_send()
    halo.wait_send()


def per_device(
    n_ep,
    n_tp,
    conv_x,
    conv_c,
    conv_b,
    conv_taps,
    w_out,
    tokens_b,
    norm_gain,
    route_b,
    route_weights,
    w_gate,
    w_up,
    w_down,
):
    n_rows, d_model = tokens_b.shape
    n_conv = conv_x.shape[0]
    cap = 2 * n_rows * TOPK // n_ep
    nz = n_ep // CORES
    far = nz // 2
    units = w_gate.shape[2]
    shares = route_weights / jnp.sum(route_weights, axis=-1, keepdims=True)
    meta = jnp.concatenate(
        [
            route_b.T.astype(F32),
            shares.T,
            jnp.zeros((META_ROWS - 2 * TOPK, n_rows), F32),
        ],
        axis=0,
    )
    wide = min(256, d_model)
    any_spec = pl.BlockSpec(memory_space=pl.ANY)
    vmem = pl.BlockSpec(memory_space=pltpu.VMEM)
    dma = pltpu.SemaphoreType.DMA
    slots = n_ep * cap
    return pl.pallas_call(
        functools.partial(fused, n_ep, n_tp, cap),
        out_shape=(
            jax.ShapeDtypeStruct((n_conv, d_model), BF16),
            jax.ShapeDtypeStruct((n_rows, d_model), BF16),
        ),
        in_specs=[any_spec, any_spec, vmem] + [any_spec] * 7 + [vmem],
        out_specs=(vmem, vmem),
        scratch_shapes=[
            pltpu.VMEM((CORES, nz, n_rows, d_model), BF16),
            pltpu.VMEM((CORES, nz, META_ROWS, n_rows), F32),
            pltpu.VMEM((n_tp, d_model, units), BF16),
            pltpu.VMEM((n_tp, d_model, units), BF16),
            pltpu.VMEM((n_tp, units, d_model), BF16),
            pltpu.VMEM((n_tp, w_out.shape[0], d_model), BF16),
            pltpu.VMEM((slots, d_model), BF16),
            pltpu.VMEM((slots, LANES), F32),
            pltpu.VMEM((slots, n_tp * units), BF16),
            pltpu.VMEM((nz, 2 * cap, d_model), BF16),
            pltpu.VMEM((nz, cap, d_model), BF16),
            pltpu.VMEM((2, far + 1, n_rows, d_model), BF16),
            pltpu.VMEM((nz, n_rows, LANES), BF16),
            pltpu.VMEM((3, n_conv, d_model), BF16),
            pltpu.VMEM((n_conv + 16, wide), F32),
            pltpu.VMEM((n_conv, d_model), BF16),
            pltpu.VMEM((16, d_model), BF16),
            pltpu.VMEM((16, d_model), BF16),
            dma((9,)),
            dma((4, 2, 2)),
            dma((4, 2, 2)),
            dma((2, far, 2)),
            dma((2, far, 2)),
            dma((2, far + 1, 2)),
            dma((2, far + 1, 2)),
            dma((2, far)),
            dma((2, far)),
            dma((2, far + 1)),
            dma((2, far + 1)),
            dma((1,)),
            dma((1,)),
            dma((2, far, 2)),
            dma((2, far, 2)),
            dma((1,)),
            dma((1,)),
        ],
        compiler_params=pltpu.CompilerParams(
            collective_id=0, has_side_effects=True, vmem_limit_bytes=67043328
        ),
    )(
        tokens_b,
        meta,
        norm_gain[None, :],
        w_gate,
        w_up,
        w_down,
        w_out,
        conv_x,
        conv_c,
        conv_b,
        conv_taps,
    )


def solution(mesh):
    rows = P(("grp", "ep", "tp"), None)
    return jax.shard_map(
        functools.partial(per_device, mesh.shape["ep"], mesh.shape["tp"]),
        mesh=mesh,
        in_specs=(
            rows,
            rows,
            rows,
            P(),
            P("tp", None),
            rows,
            P(),
            rows,
            rows,
            P("ep", None, "tp"),
            P("ep", None, "tp"),
            P("ep", "tp", None),
        ),
        out_specs=(rows, rows),
        check_vma=False,
    )
```

```python
import functools
import jax
import jax.numpy as jnp
from jax import lax
from jax.experimental import pallas as pl
from jax.experimental.pallas import tpu as pltpu
from jax.sharding import PartitionSpec as P

TOPK = 2
CORES = 2
LANES = 128
META_ROWS = 8
MESH = pl.DeviceIdType.MESH
BF16 = jnp.bfloat16
F32 = jnp.float32


def fused(
    n_ep,
    n_tp,
    cap,
    tokens,
    meta,
    gain,
    wg,
    wu,
    wd,
    wo,
    cx,
    cc,
    cb,
    taps,
    mix_out,
    exp_out,
    tok,
    meta_buf,
    gbuf,
    ubuf,
    dbuf,
    obuf,
    rows,
    wslot,
    hid,
    rcat,
    rout,
    acc,
    pt,
    conv,
    uext,
    gated,
    halo_out,
    halo_in,
    lsem,
    xs,
    xr,
    zs,
    zr,
    ps,
    pr,
    ms,
    mr,
    pms,
    pmr,
    qs,
    qr,
    rs,
    rr,
    hs,
    hr,
):
    nz = n_ep // CORES
    far = nz // 2
    ep = lax.axis_index("ep")
    tp = lax.axis_index("tp")
    z = ep // CORES
    core = ep % CORES
    n_rows = tokens.shape[0]
    d_model = tokens.shape[1]
    half = n_rows // 2

    tp_at = [{"tp": (tp + 1) % n_tp}, {"tp": (tp + n_tp - 1) % n_tp}]
    z_at = [
        {"ep": ((z + 1) % nz) * CORES + core},
        {"ep": ((z + nz - 1) % nz) * CORES + core},
    ]
    partner = {"ep": z * CORES + (1 - core)}
    lin = ep * n_tp + tp
    total = n_ep * n_tp
    after = (lin + 1) % total
    prior = (lin + total - 1) % total
    after_at = {"ep": after // n_tp, "tp": after % n_tp}
    prior_at = {"ep": prior // n_tp, "tp": prior % n_tp}

    barrier = pltpu.get_barrier_semaphore()
    peers = tp_at + z_at + [partner, after_at, prior_at]
    for peer in peers:
        pl.semaphore_signal(barrier, inc=1, device_id=peer, device_id_type=MESH)

    local = [
        pltpu.make_async_copy(tokens, tok.at[0, z], lsem.at[0]),
        pltpu.make_async_copy(meta, meta_buf.at[0, z], lsem.at[1]),
        pltpu.make_async_copy(wg.at[0], gbuf.at[tp], lsem.at[2]),
        pltpu.make_async_copy(wu.at[0], ubuf.at[tp], lsem.at[3]),
        pltpu.make_async_copy(wd.at[0], dbuf.at[tp], lsem.at[4]),
        pltpu.make_async_copy(wo, obuf.at[tp], lsem.at[5]),
        pltpu.make_async_copy(cx, conv.at[0], lsem.at[6]),
        pltpu.make_async_copy(cc, conv.at[1], lsem.at[7]),
        pltpu.make_async_copy(cb, conv.at[2], lsem.at[8]),
    ]
    for copy in local:
        copy.start()

    blocks = [(wg.at[0], gbuf), (wu.at[0], ubuf), (wd.at[0], dbuf), (wo, obuf)]

    def x_send(a, d, hop):
        src, buf = blocks[a]
        if hop == 0:
            dst = buf.at[tp]
        else:
            owner = (tp + n_tp - 1) % n_tp if d == 0 else (tp + 1) % n_tp
            part = buf.shape[1] // 2
            dst = buf.at[owner, pl.ds(d * part, part)]
            src = dst
        return pltpu.make_async_remote_copy(
            src_ref=src,
            dst_ref=dst,
            send_sem=xs.at[a, d, hop],
            recv_sem=xr.at[a, d, hop],
            device_id=tp_at[d],
            device_id_type=MESH,
        )

    def x_wait(a, d, hop):
        x_send(a, d, hop).wait_recv()

    def x_forward(a):
        for d in (0, 1):
            x_wait(a, d, 0)
            x_send(a, d, 1).start()

    def away(d, h):
        return (z + (nz - h if d == 0 else h)) % nz

    def z_send(d, h, ch):
        ref = tok.at[0, away(d, h - 1), pl.ds(ch * half, half)]
        return pltpu.make_async_remote_copy(
            src_ref=ref,
            dst_ref=ref,
            send_sem=zs.at[d, h - 1, ch],
            recv_sem=zr.at[d, h - 1, ch],
            device_id=z_at[d],
            device_id_type=MESH,
        )

    def m_send(d, h):
        ref = meta_buf.at[0, away(d, h - 1)]
        return pltpu.make_async_remote_copy(
            src_ref=ref,
            dst_ref=ref,
            send_sem=ms.at[d, h - 1],
            recv_sem=mr.at[d, h - 1],
            device_id=z_at[d],
            device_id_type=MESH,
        )

    def p_send(d, h, ch):
        at = (away(d, h), pl.ds(ch * half, half))
        return pltpu.make_async_remote_copy(
            src_ref=tok.at[(0,) + at],
            dst_ref=tok.at[(1,) + at],
            send_sem=ps.at[d, h, ch],
            recv_sem=pr.at[d, h, ch],
            device_id=partner,
            device_id_type=MESH,
        )

    def pm_send(d, h):
        at = away(d, h)
        return pltpu.make_async_remote_copy(
            src_ref=meta_buf.at[0, at],
            dst_ref=meta_buf.at[1, at],
            send_sem=pms.at[d, h],
            recv_sem=pmr.at[d, h],
            device_id=partner,
            device_id_type=MESH,
        )

    def held(d, h):
        if h == 0:
            return (0, 1) if d == 0 else ()
        return (0, 1) if h < far else (d,)

    def meta_held(d, h):
        return 0 < h < far or d == 0

    halo = pltpu.make_async_remote_copy(
        src_ref=halo_out,
        dst_ref=halo_in,
        send_sem=hs.at[0],
        recv_sem=hr.at[0],
        device_id=after_at,
        device_id_type=MESH,
    )

    tri = (
        lax.broadcasted_iota(jnp.int32, (LANES, LANES), 0)
        < lax.broadcasted_iota(jnp.int32, (LANES, LANES), 1)
    ).astype(F32).astype(BF16)

    def select(rel, zz):
        info = meta_buf[rel, zz]
        first, second = info[0:1], info[1:2]
        mine = ep.astype(F32)
        other = (z * CORES + (1 - core)).astype(F32)
        one = jnp.ones((1, LANES), F32)
        none = jnp.zeros((1, LANES), F32)
        hit = jnp.where(first == mine, one, jnp.where(second == mine, one, none))
        hit_p = jnp.where(first == other, one, jnp.where(second == other, one, none))
        share = jnp.where(
            first == mine, info[2:3], jnp.where(second == mine, info[3:4], none)
        )
        at_row = lax.broadcasted_iota(jnp.int32, (META_ROWS, LANES), 0)
        both = jnp.where(at_row == 0, hit, jnp.where(at_row == 1, hit_p, 0.0))
        rank = jnp.dot(both.astype(BF16), tri, preferred_element_type=F32)
        place = jnp.where(hit > 0, rank[0:1], -1.0)
        place_p = jnp.where(hit_p > 0, rank[1:2] + float(cap), -1.0)
        slot = lax.broadcasted_iota(jnp.int32, (LANES, LANES), 0).astype(F32)
        pick = jnp.where(slot[:cap] == place, 1.0, 0.0)
        base = pl.multiple_of((rel * nz + zz) * cap, cap)
        got = jnp.dot(pick.astype(BF16), tok[rel, zz], preferred_element_type=F32)
        mean = jnp.mean(got * got, axis=-1, keepdims=True)
        normed = got * lax.rsqrt(mean + 1e-06) * gain[...]
        rows[pl.ds(base, cap), :] = normed.astype(BF16)
        weight = jnp.sum(pick * share, axis=-1, keepdims=True)
        wslot[pl.ds(base, cap), :] = jnp.broadcast_to(weight, (cap, LANES))
        spread = jnp.where(slot == place, 1.0, jnp.where(slot == place_p, 1.0, 0.0))
        return spread

    def select_own(zz):
        pt[zz] = jnp.transpose(select(0, zz)).astype(BF16)

    def select_partner(zz):
        select(1, zz)

    local[6].wait()
    local[7].wait()
    tail = halo_out.shape[0]
    last = conv.shape[1] - tail
    halo_out[...] = (
        conv[0, pl.ds(last, tail), :].astype(F32) * conv[1, pl.ds(last, tail), :].astype(F32)
    ).astype(BF16)
    local[0].wait()
    local[1].wait()
    pl.semaphore_wait(barrier, len(peers))

    halo.start()
    for d in (0, 1):
        m_send(d, 1).start()
    for a in (0, 1, 2):
        for d in (0, 1):
            x_send(a, d, 0).start()
    for ch in (0, 1):
        for d in (0, 1):
            z_send(d, 1, ch).start()
    pm_send(0, 0).start()
    for ch in (0, 1):
        p_send(0, 0, ch).start()

    def convolve():
        local[8].wait()
        halo.wait_recv()
        n_conv = conv.shape[1]
        reach = taps.shape[0] - 1
        wide = uext.shape[1]
        edge = jnp.where(lin == 0, 0.0, 1.0)

        @pl.loop(0, d_model // wide)
        def _(n):
            cols = pl.ds(pl.multiple_of(n * wide, wide), wide)
            u = (conv[0, :, cols].astype(F32) * conv[1, :, cols].astype(F32)).astype(BF16)
            uext[pl.ds(tail, n_conv), :] = u.astype(F32)
            uext[pl.ds(0, tail), :] = halo_in[:, cols].astype(F32) * edge
            out = jnp.zeros((n_conv, wide), F32)
            for k in range(reach + 1):
                out = out + taps[pl.ds(k, 1), cols] * uext[pl.ds(tail - reach + k, n_conv), :]
            gated[:, cols] = (conv[2, :, cols].astype(F32) * out).astype(BF16)

    select_own(z)
    pm_send(0, 0).wait_recv()
    for ch in (0, 1):
        p_send(0, 0, ch).wait_recv()
    select_partner(z)

    x_at = {far // 2 - 1: (0,), far // 2 + 1: (1,), far - 1: (2,)} if far > 3 else {far - 1: (0, 1, 2)}
    for h in range(1, far + 1):
        for ch in (0, 1):
            for d in (0, 1):
                if ch in held(d, h):
                    z_send(d, h, ch).wait_recv()
                    if h < far and ch in held(d, h + 1):
                        z_send(d, h + 1, ch).start()
                    p_send(d, h, ch).start()
        for d in (0, 1):
            if meta_held(d, h):
                m_send(d, h).wait_recv()
                if h < far and meta_held(d, h + 1):
                    m_send(d, h + 1).start()
                pm_send(d, h).start()
        for a in x_at.get(h, ()):
            x_forward(a)
        if h == far - 1:
            for d in (0, 1):
                x_send(3, d, 0).start()
        if h == 1:
            convolve()
        count = 2 if h < far else 1

        @pl.loop(0, count)
        def _(k):
            select_own((z + nz + jnp.where(k == 0, -h, h)) % nz)

        for d in (0, 1):
            if meta_held(d, h):
                pm_send(d, h).wait_recv()
            for ch in held(d, h):
                p_send(d, h, ch).wait_recv()

        @pl.loop(0, count)
        def _(k):
            select_partner((z + nz + jnp.where(k == 0, -h, h)) % nz)

    local[2].wait()
    local[3].wait()
    local[4].wait()

    def hidden(step):
        b = (tp + step) % n_tp
        width = gbuf.shape[2]
        gate_val = jnp.dot(rows[...], gbuf[b], preferred_element_type=F32)
        up_val = jnp.dot(rows[...], ubuf[b], preferred_element_type=F32)
        value = gate_val / (1.0 + jnp.exp(-gate_val)) * up_val
        hid[:, pl.ds(pl.multiple_of(b * width, width), width)] = value.astype(BF16)

    @pl.loop(0, n_tp - 1)
    def _(k):
        hidden(jnp.where(k == 0, 0, jnp.where(k == 1, 1, n_tp - 1)))

    for a in (0, 1):
        for d in (0, 1):
            x_wait(a, d, 1)
    hidden(2)
    for d in (0, 1):
        x_wait(2, d, 1)
    mid = nz * cap
    depth = dbuf.shape[0] * dbuf.shape[1]

    def down(rel, n, width):
        cols = pl.ds(pl.multiple_of(n * width, width), width)
        value = jnp.dot(
            hid[pl.ds(rel * mid, mid), :],
            dbuf[:, :, cols].reshape(depth, width),
            preferred_element_type=F32,
        )
        value = (value * wslot[pl.ds(rel * mid, mid), 0:1]).astype(BF16)
        return cols, value.reshape(nz, cap, width)

    swap = pltpu.make_async_remote_copy(
        src_ref=rout,
        dst_ref=rcat.at[:, pl.ds(cap, cap), :],
        send_sem=qs.at[0],
        recv_sem=qr.at[0],
        device_id=partner,
        device_id_type=MESH,
    )
    out_wide = 512 if d_model % 512 == 0 else d_model

    @pl.loop(0, d_model // out_wide)
    def _(n):
        cols, value = down(1, n, out_wide)
        rout[:, :, cols] = value

    swap.start()

    @pl.loop(0, d_model // out_wide)
    def _(n):
        cols, value = down(0, n, out_wide)
        rcat[:, pl.ds(0, cap), cols] = value

    swap.wait_recv()

    def r_send(d, t, ch):
        at = pl.ds(ch * half, half)
        return pltpu.make_async_remote_copy(
            src_ref=acc.at[d, t - 1, at],
            dst_ref=acc.at[d, t, at],
            send_sem=rs.at[d, t - 1, ch],
            recv_sem=rr.at[d, t - 1, ch],
            device_id=z_at[d],
            device_id_type=MESH,
        )

    def spread_back(zz, ch):
        return jnp.dot(
            pt[zz, pl.ds(ch * half, half), 0 : 2 * cap],
            rcat[zz],
            preferred_element_type=F32,
        )

    def ahead(d, t):
        dist = far + 1 - t
        return (z + dist) % nz if d == 0 else (z + nz - dist) % nz

    def r_step(t, parts):
        for ch, d, arrives in parts:
            at = pl.ds(ch * half, half)
            value = spread_back(ahead(d, t), ch)
            if arrives:
                r_send(d, t - 1, ch).wait_recv()
                value = value + acc[d, t - 1, at].astype(F32)
            acc[d, t - 1, at] = value.astype(BF16)
            r_send(d, t, ch).start()

    r_step(1, [(0, 0, False), (1, 1, False)])
    r_step(2, [(0, 0, True), (1, 1, True), (1, 0, False), (0, 1, False)])
    every = [(0, 0, True), (0, 1, True), (1, 0, True), (1, 1, True)]
    turn = max(3, far - 1)

    @pl.loop(3, turn)
    def _(t):
        r_step(t, every)

    x_forward(3)

    @pl.loop(turn, far + 1)
    def _(t):
        r_step(t, every)

    for ch in (0, 1):
        at = pl.ds(ch * half, half)
        value = spread_back(z, ch)
        for d in (0, 1):
            r_send(d, far, ch).wait_recv()
            value = value + acc[d, far, at].astype(F32)
        exp_out[at, :] = value.astype(BF16)

    local[5].wait()
    for d in (0, 1):
        x_wait(3, d, 1)
    deep = obuf.shape[0] * obuf.shape[1]

    @pl.loop(0, d_model // out_wide)
    def _(n):
        cols = pl.ds(pl.multiple_of(n * out_wide, out_wide), out_wide)
        mix_out[:, cols] = jnp.dot(
            gated[...],
            obuf[:, :, cols].reshape(deep, out_wide),
            preferred_element_type=F32,
        ).astype(BF16)

    for a in range(len(blocks)):
        for d in (0, 1):
            for hop in (0, 1):
                x_send(a, d, hop).wait_send()
    for d in (0, 1):
        for h in range(far + 1):
            if h > 0:
                for ch in held(d, h):
                    z_send(d, h, ch).wait_send()
                if meta_held(d, h):
                    m_send(d, h).wait_send()
            for ch in held(d, h):
                p_send(d, h, ch).wait_send()
            if meta_held(d, h):
                pm_send(d, h).wait_send()
        for t in range(1, far + 1):
            for ch in (d,) if t == 1 else (0, 1):
                r_send(d, t, ch).wait_send()
    swap.wait_send()
    halo.wait_send()


def per_device(
    n_ep,
    n_tp,
    conv_x,
    conv_c,
    conv_b,
    conv_taps,
    w_out,
    tokens_b,
    norm_gain,
    route_b,
    route_weights,
    w_gate,
    w_up,
    w_down,
):
    n_rows, d_model = tokens_b.shape
    n_conv = conv_x.shape[0]
    cap = 2 * n_rows * TOPK // n_ep
    nz = n_ep // CORES
    far = nz // 2
    units = w_gate.shape[2]
    shares = route_weights / jnp.sum(route_weights, axis=-1, keepdims=True)
    meta = jnp.concatenate(
        [
            route_b.T.astype(F32),
            shares.T,
            jnp.zeros((META_ROWS - 2 * TOPK, n_rows), F32),
        ],
        axis=0,
    )
    wide = min(256, d_model)
    any_spec = pl.BlockSpec(memory_space=pl.ANY)
    vmem = pl.BlockSpec(memory_space=pltpu.VMEM)
    dma = pltpu.SemaphoreType.DMA
    slots = n_ep * cap
    return pl.pallas_call(
        functools.partial(fused, n_ep, n_tp, cap),
        out_shape=(
            jax.ShapeDtypeStruct((n_conv, d_model), BF16),
            jax.ShapeDtypeStruct((n_rows, d_model), BF16),
        ),
        in_specs=[any_spec, any_spec, vmem] + [any_spec] * 7 + [vmem],
        out_specs=(vmem, vmem),
        scratch_shapes=[
            pltpu.VMEM((CORES, nz, n_rows, d_model), BF16),
            pltpu.VMEM((CORES, nz, META_ROWS, n_rows), F32),
            pltpu.VMEM((n_tp, d_model, units), BF16),
            pltpu.VMEM((n_tp, d_model, units), BF16),
            pltpu.VMEM((n_tp, units, d_model), BF16),
            pltpu.VMEM((n_tp, w_out.shape[0], d_model), BF16),
            pltpu.VMEM((slots, d_model), BF16),
            pltpu.VMEM((slots, LANES), F32),
            pltpu.VMEM((slots, n_tp * units), BF16),
            pltpu.VMEM((nz, 2 * cap, d_model), BF16),
            pltpu.VMEM((nz, cap, d_model), BF16),
            pltpu.VMEM((2, far + 1, n_rows, d_model), BF16),
            pltpu.VMEM((nz, n_rows, LANES), BF16),
            pltpu.VMEM((3, n_conv, d_model), BF16),
            pltpu.VMEM((n_conv + 16, wide), F32),
            pltpu.VMEM((n_conv, d_model), BF16),
            pltpu.VMEM((16, d_model), BF16),
            pltpu.VMEM((16, d_model), BF16),
            dma((9,)),
            dma((4, 2, 2)),
            dma((4, 2, 2)),
            dma((2, far, 2)),
            dma((2, far, 2)),
            dma((2, far + 1, 2)),
            dma((2, far + 1, 2)),
            dma((2, far)),
            dma((2, far)),
            dma((2, far + 1)),
            dma((2, far + 1)),
            dma((1,)),
            dma((1,)),
            dma((2, far, 2)),
            dma((2, far, 2)),
            dma((1,)),
            dma((1,)),
        ],
        compiler_params=pltpu.CompilerParams(
            collective_id=0, has_side_effects=True, vmem_limit_bytes=67043328
        ),
    )(
        tokens_b,
        meta,
        norm_gain[None, :],
        w_gate,
        w_up,
        w_down,
        w_out,
        conv_x,
        conv_c,
        conv_b,
        conv_taps,
    )


def solution(mesh):
    rows = P(("grp", "ep", "tp"), None)
    return jax.shard_map(
        functools.partial(per_device, mesh.shape["ep"], mesh.shape["tp"]),
        mesh=mesh,
        in_specs=(
            rows,
            rows,
            rows,
            P(),
            P("tp", None),
            rows,
            P(),
            rows,
            rows,
            P("ep", None, "tp"),
            P("ep", None, "tp"),
            P("ep", "tp", None),
        ),
        out_specs=(rows, rows),
        check_vma=False,
    )
```

```python
import functools
import jax
import jax.numpy as jnp
from jax import lax
from jax.experimental import pallas as pl
from jax.experimental.pallas import tpu as pltpu
from jax.sharding import PartitionSpec as P

TOPK = 2
CORES = 2
LANES = 128
META_ROWS = 8
MESH = pl.DeviceIdType.MESH
BF16 = jnp.bfloat16
F32 = jnp.float32


def fused(
    n_ep,
    n_tp,
    cap,
    tokens,
    meta,
    gain,
    wg,
    wu,
    wd,
    wo,
    cx,
    cc,
    cb,
    taps,
    mix_out,
    exp_out,
    tok,
    meta_buf,
    gbuf,
    ubuf,
    dbuf,
    obuf,
    rows,
    wslot,
    hid,
    rcat,
    rout,
    acc,
    crecv,
    pt,
    ptf,
    conv,
    uext,
    gated,
    halo_out,
    halo_in,
    lsem,
    xs,
    xr,
    zs,
    zr,
    ps,
    pr,
    ms,
    mr,
    pms,
    pmr,
    qs,
    qr,
    fs,
    fr,
    rs,
    rr,
    hs,
    hr,
):
    nz = n_ep // CORES
    far = nz // 2
    near = far // 2
    skip = far - near
    ep = lax.axis_index("ep")
    tp = lax.axis_index("tp")
    z = ep // CORES
    core = ep % CORES
    n_rows = tokens.shape[0]
    d_model = tokens.shape[1]
    half = n_rows // 2

    tp_at = [{"tp": (tp + 1) % n_tp}, {"tp": (tp + n_tp - 1) % n_tp}]
    z_at = [
        {"ep": ((z + 1) % nz) * CORES + core},
        {"ep": ((z + nz - 1) % nz) * CORES + core},
    ]
    def z_to(d, j):
        return {"ep": ((z + (j if d == 0 else nz - j)) % nz) * CORES + core}

    partner = {"ep": z * CORES + (1 - core)}
    lin = ep * n_tp + tp
    total = n_ep * n_tp
    after = (lin + 1) % total
    prior = (lin + total - 1) % total
    after_at = {"ep": after // n_tp, "tp": after % n_tp}
    prior_at = {"ep": prior // n_tp, "tp": prior % n_tp}

    barrier = pltpu.get_barrier_semaphore()
    peers = tp_at + z_at + [partner, after_at, prior_at]
    for j in range(2, skip + 1):
        peers += [z_to(0, j), z_to(1, j)]
    for peer in peers:
        pl.semaphore_signal(barrier, inc=1, device_id=peer, device_id_type=MESH)

    local = [
        pltpu.make_async_copy(tokens, tok.at[0, z], lsem.at[0]),
        pltpu.make_async_copy(meta, meta_buf.at[0, z], lsem.at[1]),
        pltpu.make_async_copy(wg.at[0], gbuf.at[tp], lsem.at[2]),
        pltpu.make_async_copy(wu.at[0], ubuf.at[tp], lsem.at[3]),
        pltpu.make_async_copy(wd.at[0], dbuf.at[tp], lsem.at[4]),
        pltpu.make_async_copy(wo, obuf.at[tp], lsem.at[5]),
        pltpu.make_async_copy(cx, conv.at[0], lsem.at[6]),
        pltpu.make_async_copy(cc, conv.at[1], lsem.at[7]),
        pltpu.make_async_copy(cb, conv.at[2], lsem.at[8]),
    ]
    for copy in local:
        copy.start()

    blocks = [(wg.at[0], gbuf), (wu.at[0], ubuf), (wd.at[0], dbuf), (wo, obuf)]

    def x_send(a, d, hop):
        src, buf = blocks[a]
        if hop == 0:
            dst = buf.at[tp]
        else:
            owner = (tp + n_tp - 1) % n_tp if d == 0 else (tp + 1) % n_tp
            part = buf.shape[1] // 2
            dst = buf.at[owner, pl.ds(d * part, part)]
            src = dst
        return pltpu.make_async_remote_copy(
            src_ref=src,
            dst_ref=dst,
            send_sem=xs.at[a, d, hop],
            recv_sem=xr.at[a, d, hop],
            device_id=tp_at[d],
            device_id_type=MESH,
        )

    def x_wait(a, d, hop):
        x_send(a, d, hop).wait_recv()

    def x_forward(a):
        for d in (0, 1):
            x_wait(a, d, 0)
            x_send(a, d, 1).start()

    def away(d, h):
        return (z + (nz - h if d == 0 else h)) % nz

    def z_send(d, h, ch):
        ref = tok.at[0, away(d, h - 1), pl.ds(ch * half, half)]
        return pltpu.make_async_remote_copy(
            src_ref=ref,
            dst_ref=ref,
            send_sem=zs.at[d, h - 1, ch],
            recv_sem=zr.at[d, h - 1, ch],
            device_id=z_at[d],
            device_id_type=MESH,
        )

    def m_send(d, h):
        ref = meta_buf.at[0, away(d, h - 1)]
        return pltpu.make_async_remote_copy(
            src_ref=ref,
            dst_ref=ref,
            send_sem=ms.at[d, h - 1],
            recv_sem=mr.at[d, h - 1],
            device_id=z_at[d],
            device_id_type=MESH,
        )

    def p_send(d, h, ch):
        at = (away(d, h), pl.ds(ch * half, half))
        return pltpu.make_async_remote_copy(
            src_ref=tok.at[(0,) + at],
            dst_ref=tok.at[(1,) + at],
            send_sem=ps.at[d, h, ch],
            recv_sem=pr.at[d, h, ch],
            device_id=partner,
            device_id_type=MESH,
        )

    def pm_send(d, h):
        at = away(d, h)
        return pltpu.make_async_remote_copy(
            src_ref=meta_buf.at[0, at],
            dst_ref=meta_buf.at[1, at],
            send_sem=pms.at[d, h],
            recv_sem=pmr.at[d, h],
            device_id=partner,
            device_id_type=MESH,
        )

    def held(d, h):
        if h == 0:
            return (0, 1) if d == 0 else ()
        return (0, 1) if h < far else (d,)

    def meta_held(d, h):
        return 0 < h < far or d == 0

    halo = pltpu.make_async_remote_copy(
        src_ref=halo_out,
        dst_ref=halo_in,
        send_sem=hs.at[0],
        recv_sem=hr.at[0],
        device_id=after_at,
        device_id_type=MESH,
    )

    tri = (
        lax.broadcasted_iota(jnp.int32, (LANES, LANES), 0)
        < lax.broadcasted_iota(jnp.int32, (LANES, LANES), 1)
    ).astype(F32).astype(BF16)

    def select(rel, zz):
        info = meta_buf[rel, zz]
        first, second = info[0:1], info[1:2]
        mine = ep.astype(F32)
        other = (z * CORES + (1 - core)).astype(F32)
        one = jnp.ones((1, LANES), F32)
        none = jnp.zeros((1, LANES), F32)
        hit = jnp.where(first == mine, one, jnp.where(second == mine, one, none))
        hit_p = jnp.where(first == other, one, jnp.where(second == other, one, none))
        share = jnp.where(
            first == mine, info[2:3], jnp.where(second == mine, info[3:4], none)
        )
        at_row = lax.broadcasted_iota(jnp.int32, (META_ROWS, LANES), 0)
        both = jnp.where(at_row == 0, hit, jnp.where(at_row == 1, hit_p, 0.0))
        rank = jnp.dot(both.astype(BF16), tri, preferred_element_type=F32)
        place = jnp.where(hit > 0, rank[0:1], -1.0)
        place_p = jnp.where(hit_p > 0, rank[1:2] + float(cap), -1.0)
        slot = lax.broadcasted_iota(jnp.int32, (LANES, LANES), 0).astype(F32)
        pick = jnp.where(slot[:cap] == place, 1.0, 0.0)
        base = pl.multiple_of((rel * nz + zz) * cap, cap)
        got = jnp.dot(pick.astype(BF16), tok[rel, zz], preferred_element_type=F32)
        mean = jnp.mean(got * got, axis=-1, keepdims=True)
        normed = got * lax.rsqrt(mean + 1e-06) * gain[...]
        rows[pl.ds(base, cap), :] = normed.astype(BF16)
        weight = jnp.sum(pick * share, axis=-1, keepdims=True)
        wslot[pl.ds(base, cap), :] = jnp.broadcast_to(weight, (cap, LANES))
        spread = jnp.where(slot == place, 1.0, jnp.where(slot == place_p, 1.0, 0.0))
        return spread

    def spread_far(d):
        info = meta_buf[0, (z + (near if d == 0 else nz - near)) % nz]
        first, second = info[0:1], info[1:2]
        one = jnp.ones((1, LANES), F32)
        none = jnp.zeros((1, LANES), F32)
        at_row = lax.broadcasted_iota(jnp.int32, (META_ROWS, LANES), 0)
        hits = []
        for j in range(1, skip + 1):
            chip = (z + (nz - j if d == 0 else j)) % nz
            for place, index in enumerate((core, 1 - core)):
                if j < skip or place == d:
                    expert = (chip * CORES + index).astype(F32)
                    hit = jnp.where(first == expert, one, jnp.where(second == expert, one, none))
                    hits.append((hit, (j - 1) * 2 * cap + (place * cap if j < skip else 0)))
        every = jnp.zeros((META_ROWS, LANES), F32)
        for i, (hit, _) in enumerate(hits):
            every = jnp.where(at_row == i, hit, every)
        rank = jnp.dot(every.astype(BF16), tri, preferred_element_type=F32)
        slot = lax.broadcasted_iota(jnp.int32, (LANES, LANES), 0).astype(F32)
        spread = jnp.zeros((LANES, LANES), F32)
        for i, (hit, base) in enumerate(hits):
            place = jnp.where(hit > 0, rank[i : i + 1] + float(base), -1.0)
            spread = jnp.where(slot == place, 1.0, spread)
        ptf[d] = jnp.transpose(spread).astype(BF16)

    def select_own(zz):
        pt[zz] = jnp.transpose(select(0, zz)).astype(BF16)

    def select_partner(zz):
        select(1, zz)

    local[6].wait()
    local[7].wait()
    tail = halo_out.shape[0]
    last = conv.shape[1] - tail
    halo_out[...] = (
        conv[0, pl.ds(last, tail), :].astype(F32) * conv[1, pl.ds(last, tail), :].astype(F32)
    ).astype(BF16)
    local[0].wait()
    local[1].wait()
    pl.semaphore_wait(barrier, len(peers))

    halo.start()
    for d in (0, 1):
        m_send(d, 1).start()
    for a in (0, 1, 2):
        for d in (0, 1):
            x_send(a, d, 0).start()
    for ch in (0, 1):
        for d in (0, 1):
            z_send(d, 1, ch).start()
    pm_send(0, 0).start()
    for ch in (0, 1):
        p_send(0, 0, ch).start()

    def convolve():
        local[8].wait()
        halo.wait_recv()
        n_conv = conv.shape[1]
        reach = taps.shape[0] - 1
        wide = uext.shape[1]
        edge = jnp.where(lin == 0, 0.0, 1.0)

        @pl.loop(0, d_model // wide)
        def _(n):
            cols = pl.ds(pl.multiple_of(n * wide, wide), wide)
            u = (conv[0, :, cols].astype(F32) * conv[1, :, cols].astype(F32)).astype(BF16)
            uext[pl.ds(tail, n_conv), :] = u.astype(F32)
            uext[pl.ds(0, tail), :] = halo_in[:, cols].astype(F32) * edge
            out = jnp.zeros((n_conv, wide), F32)
            for k in range(reach + 1):
                out = out + taps[pl.ds(k, 1), cols] * uext[pl.ds(tail - reach + k, n_conv), :]
            gated[:, cols] = (conv[2, :, cols].astype(F32) * out).astype(BF16)

    select_own(z)
    pm_send(0, 0).wait_recv()
    for ch in (0, 1):
        p_send(0, 0, ch).wait_recv()
    select_partner(z)

    x_at = {far // 2 - 1: (0,), far // 2 + 1: (1,), far - 1: (2,)} if far > 3 else {far - 1: (0, 1, 2)}
    for h in range(1, far + 1):
        for ch in (0, 1):
            for d in (0, 1):
                if ch in held(d, h):
                    z_send(d, h, ch).wait_recv()
                    if h < far and ch in held(d, h + 1):
                        z_send(d, h + 1, ch).start()
                    p_send(d, h, ch).start()
        for d in (0, 1):
            if meta_held(d, h):
                m_send(d, h).wait_recv()
                if h < far and meta_held(d, h + 1):
                    m_send(d, h + 1).start()
                pm_send(d, h).start()
        for a in x_at.get(h, ()):
            x_forward(a)
        if h == far - 1:
            for d in (0, 1):
                x_send(3, d, 0).start()
        if h == 1:
            convolve()
        count = 2 if h < far else 1

        @pl.loop(0, count)
        def _(k):
            select_own((z + nz + jnp.where(k == 0, -h, h)) % nz)

        for d in (0, 1):
            if meta_held(d, h):
                pm_send(d, h).wait_recv()
            for ch in held(d, h):
                p_send(d, h, ch).wait_recv()

        @pl.loop(0, count)
        def _(k):
            select_partner((z + nz + jnp.where(k == 0, -h, h)) % nz)

    for d in (0, 1):
        spread_far(d)

    local[2].wait()
    local[3].wait()
    local[4].wait()

    def hidden(step):
        b = (tp + step) % n_tp
        width = gbuf.shape[2]
        gate_val = jnp.dot(rows[...], gbuf[b], preferred_element_type=F32)
        up_val = jnp.dot(rows[...], ubuf[b], preferred_element_type=F32)
        value = gate_val / (1.0 + jnp.exp(-gate_val)) * up_val
        hid[:, pl.ds(pl.multiple_of(b * width, width), width)] = value.astype(BF16)

    @pl.loop(0, n_tp - 1)
    def _(k):
        hidden(jnp.where(k == 0, 0, jnp.where(k == 1, 1, n_tp - 1)))

    for a in (0, 1):
        for d in (0, 1):
            x_wait(a, d, 1)
    hidden(2)
    for d in (0, 1):
        x_wait(2, d, 1)
    mid = nz * cap
    depth = dbuf.shape[0] * dbuf.shape[1]

    def down(rel, n, width):
        cols = pl.ds(pl.multiple_of(n * width, width), width)
        value = jnp.dot(
            hid[pl.ds(rel * mid, mid), :],
            dbuf[:, :, cols].reshape(depth, width),
            preferred_element_type=F32,
        )
        value = (value * wslot[pl.ds(rel * mid, mid), 0:1]).astype(BF16)
        return cols, value.reshape(nz, cap, width)

    swap = pltpu.make_async_remote_copy(
        src_ref=rout,
        dst_ref=rcat.at[:, pl.ds(cap, cap), :],
        send_sem=qs.at[0],
        recv_sem=qr.at[0],
        device_id=partner,
        device_id_type=MESH,
    )
    out_wide = 512 if d_model % 512 == 0 else d_model

    @pl.loop(0, d_model // out_wide)
    def _(n):
        cols, value = down(1, n, out_wide)
        rout[:, :, cols] = value

    swap.start()

    @pl.loop(0, d_model // out_wide)
    def _(n):
        cols, value = down(0, n, out_wide)
        rcat[:, pl.ds(0, cap), cols] = value

    swap.wait_recv()

    far_rows = 2 * cap * (skip - 1) + cap

    def f_send(d, j):
        zz = (z + (j + near if d == 0 else nz - j - near)) % nz
        size = 2 * cap if j < skip else cap
        return pltpu.make_async_remote_copy(
            src_ref=rcat.at[zz, pl.ds(0 if j < skip else d * cap, size)],
            dst_ref=crecv.at[d, pl.ds((j - 1) * 2 * cap, size)],
            send_sem=fs.at[d, j - 1],
            recv_sem=fr.at[d, j - 1],
            device_id=z_to(d, j),
            device_id_type=MESH,
        )

    def r_send(d, t, ch):
        at = pl.ds(ch * half, half)
        return pltpu.make_async_remote_copy(
            src_ref=acc.at[d, t - 1, at],
            dst_ref=acc.at[d, t, at],
            send_sem=rs.at[d, t - 1, ch],
            recv_sem=rr.at[d, t - 1, ch],
            device_id=z_at[d],
            device_id_type=MESH,
        )

    def spread_back(zz, ch):
        return jnp.dot(
            pt[zz, pl.ds(ch * half, half), 0 : 2 * cap],
            rcat[zz],
            preferred_element_type=F32,
        )

    def r_step(t, first):
        for ch in (0, 1):
            for d in (0, 1):
                at = pl.ds(ch * half, half)
                dist = near + 1 - t
                value = spread_back((z + (dist if d == 0 else nz - dist)) % nz, ch)
                if first:
                    value = value + jnp.dot(
                        ptf[d, at, 0:far_rows], crecv[d], preferred_element_type=F32
                    )
                else:
                    r_send(d, t - 1, ch).wait_recv()
                    value = value + acc[d, t - 1, at].astype(F32)
                acc[d, t - 1, at] = value.astype(BF16)
                r_send(d, t, ch).start()

    for j in range(skip, 0, -1):
        for d in (0, 1):
            f_send(d, j).start()
    for d in (0, 1):
        for j in range(1, skip + 1):
            f_send(d, j).wait_recv()
    r_step(1, True)
    turn = min(3, near + 1)

    @pl.loop(2, turn)
    def _(t):
        r_step(t, False)

    x_forward(3)

    @pl.loop(turn, near + 1)
    def _(t):
        r_step(t, False)

    local[5].wait()
    for d in (0, 1):
        x_wait(3, d, 1)
    deep = obuf.shape[0] * obuf.shape[1]

    @pl.loop(0, d_model // out_wide)
    def _(n):
        cols = pl.ds(pl.multiple_of(n * out_wide, out_wide), out_wide)
        mix_out[:, cols] = jnp.dot(
            gated[...],
            obuf[:, :, cols].reshape(deep, out_wide),
            preferred_element_type=F32,
        ).astype(BF16)

    for ch in (0, 1):
        at = pl.ds(ch * half, half)
        value = spread_back(z, ch)
        for d in (0, 1):
            r_send(d, near, ch).wait_recv()
            value = value + acc[d, near, at].astype(F32)
        exp_out[at, :] = value.astype(BF16)

    for a in range(len(blocks)):
        for d in (0, 1):
            for hop in (0, 1):
                x_send(a, d, hop).wait_send()
    for d in (0, 1):
        for h in range(far + 1):
            if h > 0:
                for ch in held(d, h):
                    z_send(d, h, ch).wait_send()
                if meta_held(d, h):
                    m_send(d, h).wait_send()
            for ch in held(d, h):
                p_send(d, h, ch).wait_send()
            if meta_held(d, h):
                pm_send(d, h).wait_send()
        for t in range(1, near + 1):
            for ch in (0, 1):
                r_send(d, t, ch).wait_send()
        for j in range(1, skip + 1):
            f_send(d, j).wait_send()
    swap.wait_send()
    halo.wait_send()


def per_device(
    n_ep,
    n_tp,
    conv_x,
    conv_c,
    conv_b,
    conv_taps,
    w_out,
    tokens_b,
    norm_gain,
    route_b,
    route_weights,
    w_gate,
    w_up,
    w_down,
):
    n_rows, d_model = tokens_b.shape
    n_conv = conv_x.shape[0]
    cap = 2 * n_rows * TOPK // n_ep
    nz = n_ep // CORES
    far = nz // 2
    near = far // 2
    skip = far - near
    units = w_gate.shape[2]
    shares = route_weights / jnp.sum(route_weights, axis=-1, keepdims=True)
    meta = jnp.concatenate(
        [
            route_b.T.astype(F32),
            shares.T,
            jnp.zeros((META_ROWS - 2 * TOPK, n_rows), F32),
        ],
        axis=0,
    )
    wide = min(256, d_model)
    any_spec = pl.BlockSpec(memory_space=pl.ANY)
    vmem = pl.BlockSpec(memory_space=pltpu.VMEM)
    dma = pltpu.SemaphoreType.DMA
    slots = n_ep * cap
    return pl.pallas_call(
        functools.partial(fused, n_ep, n_tp, cap),
        out_shape=(
            jax.ShapeDtypeStruct((n_conv, d_model), BF16),
            jax.ShapeDtypeStruct((n_rows, d_model), BF16),
        ),
        in_specs=[any_spec, any_spec, vmem] + [any_spec] * 7 + [vmem],
        out_specs=(vmem, vmem),
        scratch_shapes=[
            pltpu.VMEM((CORES, nz, n_rows, d_model), BF16),
            pltpu.VMEM((CORES, nz, META_ROWS, n_rows), F32),
            pltpu.VMEM((n_tp, d_model, units), BF16),
            pltpu.VMEM((n_tp, d_model, units), BF16),
            pltpu.VMEM((n_tp, units, d_model), BF16),
            pltpu.VMEM((n_tp, w_out.shape[0], d_model), BF16),
            pltpu.VMEM((slots, d_model), BF16),
            pltpu.VMEM((slots, LANES), F32),
            pltpu.VMEM((slots, n_tp * units), BF16),
            pltpu.VMEM((nz, 2 * cap, d_model), BF16),
            pltpu.VMEM((nz, cap, d_model), BF16),
            pltpu.VMEM((2, near + 1, n_rows, d_model), BF16),
            pltpu.VMEM((2, 2 * cap * (skip - 1) + cap, d_model), BF16),
            pltpu.VMEM((nz, n_rows, LANES), BF16),
            pltpu.VMEM((2, n_rows, LANES), BF16),
            pltpu.VMEM((3, n_conv, d_model), BF16),
            pltpu.VMEM((n_conv + 16, wide), F32),
            pltpu.VMEM((n_conv, d_model), BF16),
            pltpu.VMEM((16, d_model), BF16),
            pltpu.VMEM((16, d_model), BF16),
            dma((9,)),
            dma((4, 2, 2)),
            dma((4, 2, 2)),
            dma((2, far, 2)),
            dma((2, far, 2)),
            dma((2, far + 1, 2)),
            dma((2, far + 1, 2)),
            dma((2, far)),
            dma((2, far)),
            dma((2, far + 1)),
            dma((2, far + 1)),
            dma((1,)),
            dma((1,)),
            dma((2, skip)),
            dma((2, skip)),
            dma((2, near, 2)),
            dma((2, near, 2)),
            dma((1,)),
            dma((1,)),
        ],
        compiler_params=pltpu.CompilerParams(
            collective_id=0, has_side_effects=True, vmem_limit_bytes=67043328
        ),
    )(
        tokens_b,
        meta,
        norm_gain[None, :],
        w_gate,
        w_up,
        w_down,
        w_out,
        conv_x,
        conv_c,
        conv_b,
        conv_taps,
    )


def solution(mesh):
    rows = P(("grp", "ep", "tp"), None)
    return jax.shard_map(
        functools.partial(per_device, mesh.shape["ep"], mesh.shape["tp"]),
        mesh=mesh,
        in_specs=(
            rows,
            rows,
            rows,
            P(),
            P("tp", None),
            rows,
            P(),
            rows,
            rows,
            P("ep", None, "tp"),
            P("ep", None, "tp"),
            P("ep", "tp", None),
        ),
        out_specs=(rows, rows),
        check_vma=False,
    )
```

```python
import functools
import jax
import jax.numpy as jnp
from jax import lax
from jax.experimental import pallas as pl
from jax.experimental.pallas import tpu as pltpu
from jax.sharding import PartitionSpec as P

TOPK = 2
CORES = 2
LANES = 128
META_ROWS = 8
MESH = pl.DeviceIdType.MESH
BF16 = jnp.bfloat16
F32 = jnp.float32


def fused(
    n_ep,
    n_tp,
    cap,
    tokens,
    route,
    weight,
    gain,
    wg,
    wu,
    wd,
    wo,
    cx,
    cc,
    cb,
    taps,
    mix_out,
    exp_out,
    tok,
    meta_buf,
    gbuf,
    ubuf,
    dbuf,
    obuf,
    rows,
    wslot,
    hid,
    rcat,
    rout,
    acc,
    crecv,
    pt,
    ptf,
    conv,
    uext,
    gated,
    halo_out,
    halo_in,
    lsem,
    xs,
    xr,
    zs,
    zr,
    ps,
    pr,
    ms,
    mr,
    pms,
    pmr,
    qs,
    qr,
    fs,
    fr,
    rs,
    rr,
    hs,
    hr,
    osem,
    orsem,
):
    nz = n_ep // CORES
    far = nz // 2
    near = far // 2
    skip = far - near
    ep = lax.axis_index("ep")
    tp = lax.axis_index("tp")
    z = ep // CORES
    core = ep % CORES
    n_rows = tokens.shape[0]
    d_model = tokens.shape[1]
    half = n_rows // 2

    tp_at = [{"tp": (tp + 1) % n_tp}, {"tp": (tp + n_tp - 1) % n_tp}]
    z_at = [
        {"ep": ((z + 1) % nz) * CORES + core},
        {"ep": ((z + nz - 1) % nz) * CORES + core},
    ]
    def z_to(d, j):
        return {"ep": ((z + (j if d == 0 else nz - j)) % nz) * CORES + core}

    partner = {"ep": z * CORES + (1 - core)}
    lin = ep * n_tp + tp
    total = n_ep * n_tp
    after = (lin + 1) % total
    prior = (lin + total - 1) % total
    after_at = {"ep": after // n_tp, "tp": after % n_tp}
    prior_at = {"ep": prior // n_tp, "tp": prior % n_tp}

    barrier = pltpu.get_barrier_semaphore()
    peers = tp_at + z_at + [partner, after_at, prior_at]
    for j in range(2, skip + 1):
        peers += [z_to(0, j), z_to(1, j)]
    for peer in peers:
        pl.semaphore_signal(barrier, inc=1, device_id=peer, device_id_type=MESH)

    local = [
        pltpu.make_async_copy(tokens, tok.at[0, z], lsem.at[0]),
        pltpu.make_async_copy(wg.at[0], gbuf.at[tp], lsem.at[2]),
        pltpu.make_async_copy(wu.at[0], ubuf.at[tp], lsem.at[3]),
        pltpu.make_async_copy(wd.at[0], dbuf.at[tp], lsem.at[4]),
        pltpu.make_async_copy(wo, obuf.at[tp], lsem.at[5]),
        pltpu.make_async_copy(cx, conv.at[0], lsem.at[6]),
        pltpu.make_async_copy(cc, conv.at[1], lsem.at[7]),
        pltpu.make_async_copy(cb, conv.at[2], lsem.at[8]),
    ]
    for copy in local:
        copy.start()

    side = d_model // 2
    blocks = [(wg, gbuf, None), (wu, ubuf, None), (wd, dbuf, 0), (wd, dbuf, 1), (wo, obuf, None)]
    n_blocks = len(blocks)

    def x_send(a, d, hop):
        src, buf, part = blocks[a]
        cols = () if part is None else (pl.ds(part * side, side),)
        depth = buf.shape[1]
        base = 0
        if a == n_blocks - 1:
            depth = depth // CORES
            base = core * depth
        if hop == 0:
            every = (pl.ds(base, depth),)
            src = src.at[((0,) if src.shape[0] == 1 else ()) + every + cols]
            dst = buf.at[(tp,) + every + cols]
        else:
            owner = (tp + n_tp - 1) % n_tp if d == 0 else (tp + 1) % n_tp
            dst = buf.at[(owner, pl.ds(base + d * (depth // 2), depth // 2)) + cols]
            src = dst
        return pltpu.make_async_remote_copy(
            src_ref=src,
            dst_ref=dst,
            send_sem=xs.at[a, d, hop],
            recv_sem=xr.at[a, d, hop],
            device_id=tp_at[d],
            device_id_type=MESH,
        )

    def x_wait(a, d, hop):
        x_send(a, d, hop).wait_recv()

    def o_send(d, hop):
        depth = obuf.shape[1] // CORES
        if hop == 0:
            owner = (tp + n_tp - 1) % n_tp if d == 0 else (tp + 1) % n_tp
            at = (owner, pl.ds(core * depth, depth))
        else:
            at = ((tp + 2) % n_tp, pl.ds(core * depth + d * (depth // 2), depth // 2))
        return pltpu.make_async_remote_copy(
            src_ref=obuf.at[at],
            dst_ref=obuf.at[at],
            send_sem=osem.at[d, hop],
            recv_sem=orsem.at[d, hop],
            device_id=partner,
            device_id_type=MESH,
        )

    def x_forward(a):
        for d in (0, 1):
            x_wait(a, d, 0)
            x_send(a, d, 1).start()

    def away(d, h):
        return (z + (nz - h if d == 0 else h)) % nz

    def z_send(d, h, ch):
        ref = tok.at[0, away(d, h - 1), pl.ds(ch * half, half)]
        return pltpu.make_async_remote_copy(
            src_ref=ref,
            dst_ref=ref,
            send_sem=zs.at[d, h - 1, ch],
            recv_sem=zr.at[d, h - 1, ch],
            device_id=z_at[d],
            device_id_type=MESH,
        )

    def m_send(d, h):
        ref = meta_buf.at[0, away(d, h - 1)]
        return pltpu.make_async_remote_copy(
            src_ref=ref,
            dst_ref=ref,
            send_sem=ms.at[d, h - 1],
            recv_sem=mr.at[d, h - 1],
            device_id=z_at[d],
            device_id_type=MESH,
        )

    def p_send(d, h, ch):
        at = (away(d, h), pl.ds(ch * half, half))
        return pltpu.make_async_remote_copy(
            src_ref=tok.at[(0,) + at],
            dst_ref=tok.at[(1,) + at],
            send_sem=ps.at[d, h, ch],
            recv_sem=pr.at[d, h, ch],
            device_id=partner,
            device_id_type=MESH,
        )

    def pm_send(d, h):
        at = away(d, h)
        return pltpu.make_async_remote_copy(
            src_ref=meta_buf.at[0, at],
            dst_ref=meta_buf.at[1, at],
            send_sem=pms.at[d, h],
            recv_sem=pmr.at[d, h],
            device_id=partner,
            device_id_type=MESH,
        )

    def held(d, h):
        if h == 0:
            return (0, 1) if d == 0 else ()
        return (0, 1) if h < far else (d,)

    def meta_held(d, h):
        return 0 < h < far or d == 0

    halo = pltpu.make_async_remote_copy(
        src_ref=halo_out,
        dst_ref=halo_in,
        send_sem=hs.at[0],
        recv_sem=hr.at[0],
        device_id=after_at,
        device_id_type=MESH,
    )

    tri = (
        lax.broadcasted_iota(jnp.int32, (LANES, LANES), 0)
        < lax.broadcasted_iota(jnp.int32, (LANES, LANES), 1)
    ).astype(F32).astype(BF16)

    def select(rel, zz):
        info = meta_buf[rel, zz]
        first, second = info[0:1], info[1:2]
        mine = ep.astype(F32)
        other = (z * CORES + (1 - core)).astype(F32)
        one = jnp.ones((1, LANES), F32)
        none = jnp.zeros((1, LANES), F32)
        hit = jnp.where(first == mine, one, jnp.where(second == mine, one, none))
        hit_p = jnp.where(first == other, one, jnp.where(second == other, one, none))
        share = jnp.where(
            first == mine, info[2:3], jnp.where(second == mine, info[3:4], none)
        )
        at_row = lax.broadcasted_iota(jnp.int32, (META_ROWS, LANES), 0)
        both = jnp.where(at_row == 0, hit, jnp.where(at_row == 1, hit_p, 0.0))
        rank = jnp.dot(both.astype(BF16), tri, preferred_element_type=F32)
        place = jnp.where(hit > 0, rank[0:1], -1.0)
        place_p = jnp.where(hit_p > 0, rank[1:2] + float(cap), -1.0)
        slot = lax.broadcasted_iota(jnp.int32, (LANES, LANES), 0).astype(F32)
        pick = jnp.where(slot[:cap] == place, 1.0, 0.0)
        base = pl.multiple_of((rel * nz + zz) * cap, cap)
        got = jnp.dot(pick.astype(BF16), tok[rel, zz], preferred_element_type=F32)
        mean = jnp.mean(got * got, axis=-1, keepdims=True)
        normed = got * lax.rsqrt(mean + 1e-06) * gain[...]
        rows[pl.ds(base, cap), :] = normed.astype(BF16)
        weight = jnp.sum(pick * share, axis=-1, keepdims=True)
        wslot[pl.ds(base, cap), :] = jnp.broadcast_to(weight, (cap, LANES))
        spread = jnp.where(slot == place, 1.0, jnp.where(slot == place_p, 1.0, 0.0))
        return spread

    def spread_far(d):
        info = meta_buf[0, (z + (near if d == 0 else nz - near)) % nz]
        first, second = info[0:1], info[1:2]
        one = jnp.ones((1, LANES), F32)
        none = jnp.zeros((1, LANES), F32)
        at_row = lax.broadcasted_iota(jnp.int32, (META_ROWS, LANES), 0)
        hits = []
        for j in range(1, skip + 1):
            chip = (z + (nz - j if d == 0 else j)) % nz
            for place, index in enumerate((core, 1 - core)):
                if j < skip or place == d:
                    expert = (chip * CORES + index).astype(F32)
                    hit = jnp.where(first == expert, one, jnp.where(second == expert, one, none))
                    hits.append((hit, (j - 1) * 2 * cap + (place * cap if j < skip else 0)))
        every = jnp.zeros((META_ROWS, LANES), F32)
        for i, (hit, _) in enumerate(hits):
            every = jnp.where(at_row == i, hit, every)
        rank = jnp.dot(every.astype(BF16), tri, preferred_element_type=F32)
        slot = lax.broadcasted_iota(jnp.int32, (LANES, LANES), 0).astype(F32)
        spread = jnp.zeros((LANES, LANES), F32)
        for i, (hit, base) in enumerate(hits):
            place = jnp.where(hit > 0, rank[i : i + 1] + float(base), -1.0)
            spread = jnp.where(slot == place, 1.0, spread)
        ptf[d] = jnp.transpose(spread).astype(BF16)

    def select_own(zz):
        pt[zz] = jnp.transpose(select(0, zz)).astype(BF16)

    def select_partner(zz):
        select(1, zz)

    local[5].wait()
    local[6].wait()
    tail = halo_out.shape[0]
    last = conv.shape[1] - tail
    halo_out[...] = (
        conv[0, pl.ds(last, tail), :].astype(F32) * conv[1, pl.ds(last, tail), :].astype(F32)
    ).astype(BF16)
    local[0].wait()
    at_row = lax.broadcasted_iota(jnp.int32, (META_ROWS, LANES), 0)
    first, second = weight[0:1], weight[1:2]
    sums = first + second
    info = jnp.where(at_row == 2, first / sums, jnp.where(at_row == 3, second / sums, 0.0))
    info = jnp.where(at_row == 1, route[1:2].astype(F32), info)
    meta_buf[0, z] = jnp.where(at_row == 0, route[0:1].astype(F32), info)
    pl.semaphore_wait(barrier, len(peers))

    halo.start()
    for d in (0, 1):
        m_send(d, 1).start()
    for a in (0, 1, 2):
        for d in (0, 1):
            x_send(a, d, 0).start()
    for ch in (0, 1):
        for d in (0, 1):
            z_send(d, 1, ch).start()
    pm_send(0, 0).start()
    for ch in (0, 1):
        p_send(0, 0, ch).start()

    def convolve():
        local[7].wait()
        halo.wait_recv()
        n_conv = conv.shape[1]
        reach = taps.shape[0] - 1
        wide = uext.shape[1]
        edge = jnp.where(lin == 0, 0.0, 1.0)

        @pl.loop(0, d_model // wide)
        def _(n):
            cols = pl.ds(pl.multiple_of(n * wide, wide), wide)
            u = (conv[0, :, cols].astype(F32) * conv[1, :, cols].astype(F32)).astype(BF16)
            uext[pl.ds(tail, n_conv), :] = u.astype(F32)
            uext[pl.ds(0, tail), :] = halo_in[:, cols].astype(F32) * edge
            out = jnp.zeros((n_conv, wide), F32)
            for k in range(reach + 1):
                out = out + taps[pl.ds(k, 1), cols] * uext[pl.ds(tail - reach + k, n_conv), :]
            gated[:, cols] = (conv[2, :, cols].astype(F32) * out).astype(BF16)

    select_own(z)
    pm_send(0, 0).wait_recv()
    for ch in (0, 1):
        p_send(0, 0, ch).wait_recv()
    select_partner(z)

    x_at = {3: (0,), far - 4: (1,), far - 2: (2,)} if far > 7 else {far - 1: (0, 1, 2)}
    last_x = max(x_at)
    for h in range(1, far + 1):
        for ch in (0, 1):
            for d in (0, 1):
                if ch in held(d, h):
                    z_send(d, h, ch).wait_recv()
                    if h < far and ch in held(d, h + 1):
                        z_send(d, h + 1, ch).start()
                    p_send(d, h, ch).start()
        for d in (0, 1):
            if meta_held(d, h):
                m_send(d, h).wait_recv()
                if h < far and meta_held(d, h + 1):
                    m_send(d, h + 1).start()
                pm_send(d, h).start()
        for a in x_at.get(h, ()):
            x_forward(a)
        if h == last_x:
            for d in (0, 1):
                x_send(3, d, 0).start()
        if h == 1:
            convolve()
        count = 2 if h < far else 1

        @pl.loop(0, count)
        def _(k):
            select_own((z + nz + jnp.where(k == 0, -h, h)) % nz)

        for d in (0, 1):
            if meta_held(d, h):
                pm_send(d, h).wait_recv()
            for ch in held(d, h):
                p_send(d, h, ch).wait_recv()

        @pl.loop(0, count)
        def _(k):
            select_partner((z + nz + jnp.where(k == 0, -h, h)) % nz)

    for d in (0, 1):
        spread_far(d)

    local[1].wait()
    local[2].wait()
    local[3].wait()

    def hidden(step):
        b = (tp + step) % n_tp
        width = gbuf.shape[2]
        gate_val = jnp.dot(rows[...], gbuf[b], preferred_element_type=F32)
        up_val = jnp.dot(rows[...], ubuf[b], preferred_element_type=F32)
        value = gate_val / (1.0 + jnp.exp(-gate_val)) * up_val
        hid[:, pl.ds(pl.multiple_of(b * width, width), width)] = value.astype(BF16)

    @pl.loop(0, n_tp - 1)
    def _(k):
        hidden(jnp.where(k == 0, 0, jnp.where(k == 1, 1, n_tp - 1)))

    for a in (0, 1):
        for d in (0, 1):
            x_wait(a, d, 1)
    hidden(2)
    mid = nz * cap
    depth = dbuf.shape[0] * dbuf.shape[1]
    out_wide = min(512, side)

    def down(rel, n, width):
        cols = pl.ds(pl.multiple_of(n * width, width), width)
        value = jnp.dot(
            hid[pl.ds(rel * mid, mid), :],
            dbuf[:, :, cols].reshape(depth, width),
            preferred_element_type=F32,
        )
        value = (value * wslot[pl.ds(rel * mid, mid), 0:1]).astype(BF16)
        return cols, value.reshape(nz, cap, width)

    def swap(ch):
        cols = pl.ds(ch * side, side)
        return pltpu.make_async_remote_copy(
            src_ref=rout.at[:, :, cols],
            dst_ref=rcat.at[:, pl.ds(cap, cap), cols],
            send_sem=qs.at[ch],
            recv_sem=qr.at[ch],
            device_id=partner,
            device_id_type=MESH,
        )

    def results(ch):
        tiles = side // out_wide

        @pl.loop(ch * tiles, (ch + 1) * tiles)
        def _(n):
            cols, value = down(1, n, out_wide)
            rout[:, :, cols] = value

        swap(ch).start()

        @pl.loop(ch * tiles, (ch + 1) * tiles)
        def _(n):
            cols, value = down(0, n, out_wide)
            rcat[:, pl.ds(0, cap), cols] = value

        swap(ch).wait_recv()

    far_rows = 2 * cap * (skip - 1) + cap

    def f_send(d, j, ch):
        zz = (z + (j + near if d == 0 else nz - j - near)) % nz
        size = 2 * cap if j < skip else cap
        cols = pl.ds(ch * side, side)
        return pltpu.make_async_remote_copy(
            src_ref=rcat.at[zz, pl.ds(0 if j < skip else d * cap, size), cols],
            dst_ref=crecv.at[d, pl.ds((j - 1) * 2 * cap, size), cols],
            send_sem=fs.at[d, j - 1, ch],
            recv_sem=fr.at[d, j - 1, ch],
            device_id=z_to(d, j),
            device_id_type=MESH,
        )

    def r_send(d, t, ch):
        cols = pl.ds(ch * side, side)
        return pltpu.make_async_remote_copy(
            src_ref=acc.at[d, t - 1, :, cols],
            dst_ref=acc.at[d, t, :, cols],
            send_sem=rs.at[d, t - 1, ch],
            recv_sem=rr.at[d, t - 1, ch],
            device_id=z_at[d],
            device_id_type=MESH,
        )

    def spread_back(zz, ch):
        return jnp.dot(
            pt[zz, :, 0 : 2 * cap],
            rcat[zz, :, pl.ds(ch * side, side)],
            preferred_element_type=F32,
        )

    def r_step(t, ch, first):
        cols = pl.ds(ch * side, side)
        for d in (0, 1):
            dist = near + 1 - t
            value = spread_back((z + (dist if d == 0 else nz - dist)) % nz, ch)
            if first:
                for j in range(1, skip + 1):
                    f_send(d, j, ch).wait_recv()
                value = value + jnp.dot(
                    ptf[d, :, 0:far_rows], crecv[d, :, cols], preferred_element_type=F32
                )
            else:
                r_send(d, t - 1, ch).wait_recv()
                value = value + acc[d, t - 1, :, cols].astype(F32)
            acc[d, t - 1, :, cols] = value.astype(BF16)
            r_send(d, t, ch).start()

    def far_out(ch):
        for j in range(skip, 0, -1):
            for d in (0, 1):
                f_send(d, j, ch).start()

    for d in (0, 1):
        x_wait(2, d, 1)
    results(0)
    far_out(0)
    x_forward(3)
    for d in (0, 1):
        x_send(4, d, 0).start()
    for d in (0, 1):
        x_wait(3, d, 1)
    results(1)
    far_out(1)
    r_step(1, 0, True)
    r_step(1, 1, True)
    turn = min(3, near + 1)

    @pl.loop(2, turn)
    def _(t):
        r_step(t, 0, False)
        r_step(t, 1, False)

    x_forward(4)
    for d in (0, 1):
        o_send(d, 0).start()

    @pl.loop(turn, near + 1)
    def _(t):
        r_step(t, 0, False)
        r_step(t, 1, False)

    local[4].wait()
    for d in (0, 1):
        x_wait(4, d, 1)
        o_send(d, 1).start()
    for d in (0, 1):
        for hop in (0, 1):
            o_send(d, hop).wait_recv()
    deep = obuf.shape[0] * obuf.shape[1]

    @pl.loop(0, d_model // out_wide)
    def _(n):
        cols = pl.ds(pl.multiple_of(n * out_wide, out_wide), out_wide)
        mix_out[:, cols] = jnp.dot(
            gated[...],
            obuf[:, :, cols].reshape(deep, out_wide),
            preferred_element_type=F32,
        ).astype(BF16)

    for ch in (0, 1):
        cols = pl.ds(ch * side, side)
        value = spread_back(z, ch)
        for d in (0, 1):
            r_send(d, near, ch).wait_recv()
            value = value + acc[d, near, :, cols].astype(F32)
        exp_out[:, cols] = value.astype(BF16)

    for a in range(n_blocks):
        for d in (0, 1):
            for hop in (0, 1):
                x_send(a, d, hop).wait_send()
    for d in (0, 1):
        for h in range(far + 1):
            if h > 0:
                for ch in held(d, h):
                    z_send(d, h, ch).wait_send()
                if meta_held(d, h):
                    m_send(d, h).wait_send()
            for ch in held(d, h):
                p_send(d, h, ch).wait_send()
            if meta_held(d, h):
                pm_send(d, h).wait_send()
        for t in range(1, near + 1):
            for ch in (0, 1):
                r_send(d, t, ch).wait_send()
        for j in range(1, skip + 1):
            for ch in (0, 1):
                f_send(d, j, ch).wait_send()
    for ch in (0, 1):
        swap(ch).wait_send()
    for d in (0, 1):
        for hop in (0, 1):
            o_send(d, hop).wait_send()
    halo.wait_send()


def per_device(
    n_ep,
    n_tp,
    conv_x,
    conv_c,
    conv_b,
    conv_taps,
    w_out,
    tokens_b,
    norm_gain,
    route_b,
    route_weights,
    w_gate,
    w_up,
    w_down,
):
    n_rows, d_model = tokens_b.shape
    n_conv = conv_x.shape[0]
    cap = 2 * n_rows * TOPK // n_ep
    nz = n_ep // CORES
    far = nz // 2
    near = far // 2
    skip = far - near
    units = w_gate.shape[2]
    wide = min(256, d_model)
    any_spec = pl.BlockSpec(memory_space=pl.ANY)
    vmem = pl.BlockSpec(memory_space=pltpu.VMEM)
    dma = pltpu.SemaphoreType.DMA
    slots = n_ep * cap
    return pl.pallas_call(
        functools.partial(fused, n_ep, n_tp, cap),
        out_shape=(
            jax.ShapeDtypeStruct((n_conv, d_model), BF16),
            jax.ShapeDtypeStruct((n_rows, d_model), BF16),
        ),
        in_specs=[any_spec, vmem, vmem, vmem] + [any_spec] * 7 + [vmem],
        out_specs=(vmem, vmem),
        scratch_shapes=[
            pltpu.VMEM((CORES, nz, n_rows, d_model), BF16),
            pltpu.VMEM((CORES, nz, META_ROWS, n_rows), F32),
            pltpu.VMEM((n_tp, d_model, units), BF16),
            pltpu.VMEM((n_tp, d_model, units), BF16),
            pltpu.VMEM((n_tp, units, d_model), BF16),
            pltpu.VMEM((n_tp, w_out.shape[0], d_model), BF16),
            pltpu.VMEM((slots, d_model), BF16),
            pltpu.VMEM((slots, LANES), F32),
            pltpu.VMEM((slots, n_tp * units), BF16),
            pltpu.VMEM((nz, 2 * cap, d_model), BF16),
            pltpu.VMEM((nz, cap, d_model), BF16),
            pltpu.VMEM((2, near + 1, n_rows, d_model), BF16),
            pltpu.VMEM((2, 2 * cap * (skip - 1) + cap, d_model), BF16),
            pltpu.VMEM((nz, n_rows, LANES), BF16),
            pltpu.VMEM((2, n_rows, LANES), BF16),
            pltpu.VMEM((3, n_conv, d_model), BF16),
            pltpu.VMEM((n_conv + 16, wide), F32),
            pltpu.VMEM((n_conv, d_model), BF16),
            pltpu.VMEM((16, d_model), BF16),
            pltpu.VMEM((16, d_model), BF16),
            dma((9,)),
            dma((5, 2, 2)),
            dma((5, 2, 2)),
            dma((2, far, 2)),
            dma((2, far, 2)),
            dma((2, far + 1, 2)),
            dma((2, far + 1, 2)),
            dma((2, far)),
            dma((2, far)),
            dma((2, far + 1)),
            dma((2, far + 1)),
            dma((2,)),
            dma((2,)),
            dma((2, skip, 2)),
            dma((2, skip, 2)),
            dma((2, near, 2)),
            dma((2, near, 2)),
            dma((1,)),
            dma((1,)),
            dma((2, 2)),
            dma((2, 2)),
        ],
        compiler_params=pltpu.CompilerParams(
            collective_id=0, has_side_effects=True, vmem_limit_bytes=67043328
        ),
    )(
        tokens_b,
        route_b.T,
        route_weights.T,
        norm_gain[None, :],
        w_gate,
        w_up,
        w_down,
        w_out,
        conv_x,
        conv_c,
        conv_b,
        conv_taps,
    )


def solution(mesh):
    rows = P(("grp", "ep", "tp"), None)
    return jax.shard_map(
        functools.partial(per_device, mesh.shape["ep"], mesh.shape["tp"]),
        mesh=mesh,
        in_specs=(
            rows,
            rows,
            rows,
            P(),
            P("tp", None),
            rows,
            P(),
            rows,
            rows,
            P("ep", None, "tp"),
            P("ep", None, "tp"),
            P("ep", "tp", None),
        ),
        out_specs=(rows, rows),
        check_vma=False,
    )
```

```python
import functools
import jax
import jax.numpy as jnp
from jax import lax
from jax.experimental import pallas as pl
from jax.experimental.pallas import tpu as pltpu
from jax.sharding import PartitionSpec as P

TOPK = 2
CORES = 2
LANES = 128
META_ROWS = 8
MESH = pl.DeviceIdType.MESH
BF16 = jnp.bfloat16
F32 = jnp.float32


def fused(
    n_ep,
    n_tp,
    cap,
    tokens,
    route,
    weight,
    gain,
    wg,
    wu,
    wd,
    wo,
    cx,
    cc,
    cb,
    taps,
    mix_out,
    exp_out,
    tok,
    meta_buf,
    gbuf,
    ubuf,
    dbuf,
    obuf,
    rows,
    wslot,
    hid,
    rcat,
    rout,
    acc,
    crecv,
    gsend,
    grecv,
    gother,
    pt,
    ptf,
    conv,
    uext,
    gated,
    halo_out,
    halo_in,
    lsem,
    xs,
    xr,
    zs,
    zr,
    ps,
    pr,
    ms,
    mr,
    pms,
    pmr,
    qs,
    qr,
    fs,
    fr,
    rs,
    rr,
    hs,
    hr,
    osem,
    orsem,
    gs,
    gr,
    gps,
    gpr,
):
    nz = n_ep // CORES
    far = nz // 2
    near = far // 2
    skip = far - near
    ep = lax.axis_index("ep")
    tp = lax.axis_index("tp")
    z = ep // CORES
    core = ep % CORES
    n_rows = tokens.shape[0]
    d_model = tokens.shape[1]
    half = n_rows // 2

    tp_at = [{"tp": (tp + 1) % n_tp}, {"tp": (tp + n_tp - 1) % n_tp}]
    z_at = [
        {"ep": ((z + 1) % nz) * CORES + core},
        {"ep": ((z + nz - 1) % nz) * CORES + core},
    ]
    def z_to(d, j):
        return {"ep": ((z + (j if d == 0 else nz - j)) % nz) * CORES + core}

    partner = {"ep": z * CORES + (1 - core)}
    lin = ep * n_tp + tp
    total = n_ep * n_tp
    after = (lin + 1) % total
    prior = (lin + total - 1) % total
    after_at = {"ep": after // n_tp, "tp": after % n_tp}
    prior_at = {"ep": prior // n_tp, "tp": prior % n_tp}

    barrier = pltpu.get_barrier_semaphore()
    peers = tp_at + z_at + [partner, after_at, prior_at]
    for j in range(2, skip + 1):
        peers += [z_to(0, j), z_to(1, j)]
    for peer in peers:
        pl.semaphore_signal(barrier, inc=1, device_id=peer, device_id_type=MESH)

    local = [
        pltpu.make_async_copy(tokens, tok.at[0, z], lsem.at[0]),
        pltpu.make_async_copy(wg.at[0], gbuf.at[tp], lsem.at[2]),
        pltpu.make_async_copy(wu.at[0], ubuf.at[tp], lsem.at[3]),
        pltpu.make_async_copy(wd.at[0], dbuf.at[tp], lsem.at[4]),
        pltpu.make_async_copy(wo, obuf.at[tp], lsem.at[5]),
        pltpu.make_async_copy(cx, conv.at[0], lsem.at[6]),
        pltpu.make_async_copy(cc, conv.at[1], lsem.at[7]),
        pltpu.make_async_copy(cb, conv.at[2], lsem.at[8]),
    ]
    for copy in local:
        copy.start()

    quarter = d_model // 4
    parts = [(0, quarter), (quarter, quarter), (2 * quarter, 2 * quarter)]
    n_parts = len(parts)
    blocks = [(wg, gbuf, None), (wu, ubuf, None)]
    blocks += [(wd, dbuf, k) for k in range(n_parts)] + [(wo, obuf, None)]
    n_blocks = len(blocks)

    def x_send(a, d, hop):
        src, buf, part = blocks[a]
        cols = () if part is None else (pl.ds(*parts[part]),)
        depth = buf.shape[1]
        base = 0
        if a == n_blocks - 1:
            depth = depth // CORES
            base = core * depth
        if hop == 0:
            every = (pl.ds(base, depth),)
            src = src.at[((0,) if src.shape[0] == 1 else ()) + every + cols]
            dst = buf.at[(tp,) + every + cols]
        else:
            owner = (tp + n_tp - 1) % n_tp if d == 0 else (tp + 1) % n_tp
            dst = buf.at[(owner, pl.ds(base + d * (depth // 2), depth // 2)) + cols]
            src = dst
        return pltpu.make_async_remote_copy(
            src_ref=src,
            dst_ref=dst,
            send_sem=xs.at[a, d, hop],
            recv_sem=xr.at[a, d, hop],
            device_id=tp_at[d],
            device_id_type=MESH,
        )

    def x_wait(a, d, hop):
        x_send(a, d, hop).wait_recv()

    def o_send(d, hop):
        depth = obuf.shape[1] // CORES
        if hop == 0:
            owner = (tp + n_tp - 1) % n_tp if d == 0 else (tp + 1) % n_tp
            at = (owner, pl.ds(core * depth, depth))
        else:
            at = ((tp + 2) % n_tp, pl.ds(core * depth + d * (depth // 2), depth // 2))
        return pltpu.make_async_remote_copy(
            src_ref=obuf.at[at],
            dst_ref=obuf.at[at],
            send_sem=osem.at[d, hop],
            recv_sem=orsem.at[d, hop],
            device_id=partner,
            device_id_type=MESH,
        )

    def x_forward(a):
        for d in (0, 1):
            x_wait(a, d, 0)
            x_send(a, d, 1).start()

    def away(d, h):
        return (z + (nz - h if d == 0 else h)) % nz

    def z_send(d, h, ch):
        ref = tok.at[0, away(d, h - 1), pl.ds(ch * half, half)]
        return pltpu.make_async_remote_copy(
            src_ref=ref,
            dst_ref=ref,
            send_sem=zs.at[d, h - 1, ch],
            recv_sem=zr.at[d, h - 1, ch],
            device_id=z_at[d],
            device_id_type=MESH,
        )

    def m_send(d, h):
        ref = meta_buf.at[0, z if h <= near else away(d, near)]
        return pltpu.make_async_remote_copy(
            src_ref=ref,
            dst_ref=ref,
            send_sem=ms.at[d, h - 1],
            recv_sem=mr.at[d, h - 1],
            device_id=z_to(d, h if h <= near else h - near),
            device_id_type=MESH,
        )

    far_rows = 2 * cap * (skip - 1) + cap

    def g_send(d, j):
        at = pl.ds((j - 1) * 2 * cap, 2 * cap if j < skip else cap)
        return pltpu.make_async_remote_copy(
            src_ref=gsend.at[d, at],
            dst_ref=grecv.at[d, at],
            send_sem=gs.at[d, j - 1],
            recv_sem=gr.at[d, j - 1],
            device_id=z_to(d, j),
            device_id_type=MESH,
        )

    def gp_send(d, j):
        base = (j - 1) * 2 * cap + (cap if j < skip else 0)
        return pltpu.make_async_remote_copy(
            src_ref=grecv.at[d, pl.ds(base, cap)],
            dst_ref=gother.at[d, j - 1],
            send_sem=gps.at[d, j - 1],
            recv_sem=gpr.at[d, j - 1],
            device_id=partner,
            device_id_type=MESH,
        )

    def p_send(d, h, ch):
        at = (away(d, h), pl.ds(ch * half, half))
        return pltpu.make_async_remote_copy(
            src_ref=tok.at[(0,) + at],
            dst_ref=tok.at[(1,) + at],
            send_sem=ps.at[d, h, ch],
            recv_sem=pr.at[d, h, ch],
            device_id=partner,
            device_id_type=MESH,
        )

    def pm_send(d, h):
        at = away(d, h)
        return pltpu.make_async_remote_copy(
            src_ref=meta_buf.at[0, at],
            dst_ref=meta_buf.at[1, at],
            send_sem=pms.at[d, h],
            recv_sem=pmr.at[d, h],
            device_id=partner,
            device_id_type=MESH,
        )

    def held(d, h):
        if h == 0:
            return (0, 1) if d == 0 else ()
        return (0, 1) if h <= near else ()

    def meta_held(d, h):
        return 0 < h < far or d == 0

    halo = pltpu.make_async_remote_copy(
        src_ref=halo_out,
        dst_ref=halo_in,
        send_sem=hs.at[0],
        recv_sem=hr.at[0],
        device_id=after_at,
        device_id_type=MESH,
    )

    tri = (
        lax.broadcasted_iota(jnp.int32, (LANES, LANES), 0)
        < lax.broadcasted_iota(jnp.int32, (LANES, LANES), 1)
    ).astype(F32).astype(BF16)

    def select(rel, zz, arrived=None):
        info = meta_buf[rel, zz]
        first, second = info[0:1], info[1:2]
        mine = ep.astype(F32)
        other = (z * CORES + (1 - core)).astype(F32)
        one = jnp.ones((1, LANES), F32)
        none = jnp.zeros((1, LANES), F32)
        hit = jnp.where(first == mine, one, jnp.where(second == mine, one, none))
        hit_p = jnp.where(first == other, one, jnp.where(second == other, one, none))
        share = jnp.where(
            first == mine, info[2:3], jnp.where(second == mine, info[3:4], none)
        )
        at_row = lax.broadcasted_iota(jnp.int32, (META_ROWS, LANES), 0)
        both = jnp.where(at_row == 0, hit, jnp.where(at_row == 1, hit_p, 0.0))
        rank = jnp.dot(both.astype(BF16), tri, preferred_element_type=F32)
        place = jnp.where(hit > 0, rank[0:1], -1.0)
        place_p = jnp.where(hit_p > 0, rank[1:2] + float(cap), -1.0)
        slot = lax.broadcasted_iota(jnp.int32, (LANES, LANES), 0).astype(F32)
        pick = jnp.where(slot[:cap] == place, 1.0, 0.0)
        base = pl.multiple_of((rel * nz + zz) * cap, cap)
        if arrived is None:
            got = jnp.dot(pick.astype(BF16), tok[rel, zz], preferred_element_type=F32)
        else:
            got = arrived.astype(F32)
        mean = jnp.mean(got * got, axis=-1, keepdims=True)
        normed = got * lax.rsqrt(mean + 1e-06) * gain[...]
        rows[pl.ds(base, cap), :] = normed.astype(BF16)
        weight = jnp.sum(pick * share, axis=-1, keepdims=True)
        wslot[pl.ds(base, cap), :] = jnp.broadcast_to(weight, (cap, LANES))
        spread = jnp.where(slot == place, 1.0, jnp.where(slot == place_p, 1.0, 0.0))
        return spread

    def slot_rows(info, d, ahead):
        first, second = info[0:1], info[1:2]
        one = jnp.ones((1, LANES), F32)
        none = jnp.zeros((1, LANES), F32)
        at_row = lax.broadcasted_iota(jnp.int32, (META_ROWS, LANES), 0)
        hits = []
        for j in range(1, skip + 1):
            chip = (z + (j if (d == 0) == ahead else nz - j)) % nz
            for place, index in enumerate((core, 1 - core)):
                if j < skip or place == d:
                    expert = (chip * CORES + index).astype(F32)
                    hit = jnp.where(first == expert, one, jnp.where(second == expert, one, none))
                    hits.append((hit, (j - 1) * 2 * cap + (place * cap if j < skip else 0)))
        every = jnp.zeros((META_ROWS, LANES), F32)
        for i, (hit, _) in enumerate(hits):
            every = jnp.where(at_row == i, hit, every)
        rank = jnp.dot(every.astype(BF16), tri, preferred_element_type=F32)
        slot = lax.broadcasted_iota(jnp.int32, (LANES, LANES), 0).astype(F32)
        spread = jnp.zeros((LANES, LANES), F32)
        for i, (hit, base) in enumerate(hits):
            place = jnp.where(hit > 0, rank[i : i + 1] + float(base), -1.0)
            spread = jnp.where(slot == place, 1.0, spread)
        return spread

    def spread_far(d):
        info = meta_buf[0, (z + (near if d == 0 else nz - near)) % nz]
        ptf[d] = jnp.transpose(slot_rows(info, d, False)).astype(BF16)

    def compact(d):
        source = away(d, near)
        pick = slot_rows(meta_buf[0, source], d, True)[:far_rows]
        got = jnp.dot(pick.astype(BF16), tok[0, source], preferred_element_type=F32)
        gsend[d] = got.astype(BF16)

    def select_own(zz, arrived=None):
        pt[zz] = jnp.transpose(select(0, zz, arrived)).astype(BF16)

    def select_partner(zz, arrived=None):
        select(1, zz, arrived)

    local[5].wait()
    local[6].wait()
    tail = halo_out.shape[0]
    last = conv.shape[1] - tail
    halo_out[...] = (
        conv[0, pl.ds(last, tail), :].astype(F32) * conv[1, pl.ds(last, tail), :].astype(F32)
    ).astype(BF16)
    local[0].wait()
    at_row = lax.broadcasted_iota(jnp.int32, (META_ROWS, LANES), 0)
    first, second = weight[0:1], weight[1:2]
    sums = first + second
    info = jnp.where(at_row == 2, first / sums, jnp.where(at_row == 3, second / sums, 0.0))
    info = jnp.where(at_row == 1, route[1:2].astype(F32), info)
    meta_buf[0, z] = jnp.where(at_row == 0, route[0:1].astype(F32), info)
    pl.semaphore_wait(barrier, len(peers))

    halo.start()
    for h in range(1, near + 1):
        for d in (0, 1):
            m_send(d, h).start()
    for a in (0, 1, 2):
        for d in (0, 1):
            x_send(a, d, 0).start()
    for ch in (0, 1):
        for d in (0, 1):
            z_send(d, 1, ch).start()
    pm_send(0, 0).start()
    for ch in (0, 1):
        p_send(0, 0, ch).start()
    for d in (0, 1):
        m_send(d, near).wait_recv()
        pm_send(d, near).start()
    for j in range(1, skip + 1):
        for d in (0, 1):
            if meta_held(d, near + j):
                m_send(d, near + j).start()

    def convolve():
        local[7].wait()
        halo.wait_recv()
        n_conv = conv.shape[1]
        reach = taps.shape[0] - 1
        wide = uext.shape[1]
        edge = jnp.where(lin == 0, 0.0, 1.0)

        @pl.loop(0, d_model // wide)
        def _(n):
            cols = pl.ds(pl.multiple_of(n * wide, wide), wide)
            u = (conv[0, :, cols].astype(F32) * conv[1, :, cols].astype(F32)).astype(BF16)
            uext[pl.ds(tail, n_conv), :] = u.astype(F32)
            uext[pl.ds(0, tail), :] = halo_in[:, cols].astype(F32) * edge
            out = jnp.zeros((n_conv, wide), F32)
            for k in range(reach + 1):
                out = out + taps[pl.ds(k, 1), cols] * uext[pl.ds(tail - reach + k, n_conv), :]
            gated[:, cols] = (conv[2, :, cols].astype(F32) * out).astype(BF16)

    select_own(z)
    pm_send(0, 0).wait_recv()
    for ch in (0, 1):
        p_send(0, 0, ch).wait_recv()
    select_partner(z)

    for h in range(1, near + 1):
        for d in (0, 1):
            if h < near:
                m_send(d, h).wait_recv()
                pm_send(d, h).start()
        for ch in (0, 1):
            for d in (0, 1):
                z_send(d, h, ch).wait_recv()
                if h < near:
                    z_send(d, h + 1, ch).start()
                p_send(d, h, ch).start()
        if h == near:
            for d in (0, 1):
                compact(d)
                for j in range(skip, 0, -1):
                    g_send(d, j).start()
        if h == min(3, near):
            x_forward(0)
        if h == near:
            x_forward(1)
        if h == 1:
            convolve()

        @pl.loop(0, 2)
        def _(k):
            select_own((z + nz + jnp.where(k == 0, -h, h)) % nz)

        for d in (0, 1):
            pm_send(d, h).wait_recv()
            for ch in (0, 1):
                p_send(d, h, ch).wait_recv()

        @pl.loop(0, 2)
        def _(k):
            select_partner((z + nz + jnp.where(k == 0, -h, h)) % nz)

    for j in range(1, skip + 1):
        for d in (0, 1):
            if meta_held(d, near + j):
                m_send(d, near + j).wait_recv()
                pm_send(d, near + j).start()
    x_forward(2)
    for k in range(1, n_parts):
        for d in (0, 1):
            x_send(2 + k, d, 0).start()
    for d in (0, 1):
        spread_far(d)
    for j in range(1, skip + 1):
        for d in (0, 1):
            g_send(d, j).wait_recv()
            if j < skip or d == 1:
                gp_send(d, j).start()
            if j < skip or d == 0:
                select_own(away(d, near + j), grecv[d, pl.ds((j - 1) * 2 * cap, cap), :])
    for j in range(1, skip + 1):
        for d in (0, 1):
            if meta_held(d, near + j):
                pm_send(d, near + j).wait_recv()
            if j < skip or d == 1:
                gp_send(d, j).wait_recv()
    for j in range(1, skip + 1):
        for d in (0, 1):
            if j < skip or d == 1:
                select_partner(away(d, near + j), gother[d, j - 1])

    local[1].wait()
    local[2].wait()
    local[3].wait()

    def hidden(step):
        b = (tp + step) % n_tp
        width = gbuf.shape[2]
        gate_val = jnp.dot(rows[...], gbuf[b], preferred_element_type=F32)
        up_val = jnp.dot(rows[...], ubuf[b], preferred_element_type=F32)
        value = gate_val / (1.0 + jnp.exp(-gate_val)) * up_val
        hid[:, pl.ds(pl.multiple_of(b * width, width), width)] = value.astype(BF16)

    @pl.loop(0, n_tp - 1)
    def _(k):
        hidden(jnp.where(k == 0, 0, jnp.where(k == 1, 1, n_tp - 1)))

    for a in (0, 1):
        for d in (0, 1):
            x_wait(a, d, 1)
    hidden(2)
    mid = nz * cap
    depth = dbuf.shape[0] * dbuf.shape[1]
    out_wide = min(512, quarter)

    def down(rel, n, width):
        cols = pl.ds(pl.multiple_of(n * width, width), width)
        value = jnp.dot(
            hid[pl.ds(rel * mid, mid), :],
            dbuf[:, :, cols].reshape(depth, width),
            preferred_element_type=F32,
        )
        value = (value * wslot[pl.ds(rel * mid, mid), 0:1]).astype(BF16)
        return cols, value.reshape(nz, cap, width)

    def swap(ch):
        cols = pl.ds(*parts[ch])
        return pltpu.make_async_remote_copy(
            src_ref=rout.at[:, :, cols],
            dst_ref=rcat.at[:, pl.ds(cap, cap), cols],
            send_sem=qs.at[ch],
            recv_sem=qr.at[ch],
            device_id=partner,
            device_id_type=MESH,
        )

    def results(ch):
        low = parts[ch][0] // out_wide
        high = low + parts[ch][1] // out_wide

        @pl.loop(low, high)
        def _(n):
            cols, value = down(1, n, out_wide)
            rout[:, :, cols] = value

        swap(ch).start()

        @pl.loop(low, high)
        def _(n):
            cols, value = down(0, n, out_wide)
            rcat[:, pl.ds(0, cap), cols] = value

        swap(ch).wait_recv()

    def f_send(d, j, ch):
        zz = (z + (j + near if d == 0 else nz - j - near)) % nz
        size = 2 * cap if j < skip else cap
        cols = pl.ds(*parts[ch])
        return pltpu.make_async_remote_copy(
            src_ref=rcat.at[zz, pl.ds(0 if j < skip else d * cap, size), cols],
            dst_ref=crecv.at[d, pl.ds((j - 1) * 2 * cap, size), cols],
            send_sem=fs.at[d, j - 1, ch],
            recv_sem=fr.at[d, j - 1, ch],
            device_id=z_to(d, j),
            device_id_type=MESH,
        )

    def r_send(d, t, ch):
        cols = pl.ds(*parts[ch])
        return pltpu.make_async_remote_copy(
            src_ref=acc.at[d, t - 1, :, cols],
            dst_ref=acc.at[d, t, :, cols],
            send_sem=rs.at[d, t - 1, ch],
            recv_sem=rr.at[d, t - 1, ch],
            device_id=z_at[d],
            device_id_type=MESH,
        )

    def spread_back(zz, ch):
        return jnp.dot(
            pt[zz, :, 0 : 2 * cap],
            rcat[zz, :, pl.ds(*parts[ch])],
            preferred_element_type=F32,
        )

    def r_step(t, ch, first):
        cols = pl.ds(*parts[ch])
        for d in (0, 1):
            dist = near + 1 - t
            value = spread_back((z + (dist if d == 0 else nz - dist)) % nz, ch)
            if first:
                for j in range(1, skip + 1):
                    f_send(d, j, ch).wait_recv()
                value = value + jnp.dot(
                    ptf[d, :, 0:far_rows], crecv[d, :, cols], preferred_element_type=F32
                )
            else:
                r_send(d, t - 1, ch).wait_recv()
                value = value + acc[d, t - 1, :, cols].astype(F32)
            acc[d, t - 1, :, cols] = value.astype(BF16)
            r_send(d, t, ch).start()

    def far_out(ch):
        for j in range(skip, 0, -1):
            for d in (0, 1):
                f_send(d, j, ch).start()

    for d in (0, 1):
        x_wait(2, d, 1)
    results(0)
    far_out(0)
    for k in range(1, n_parts):
        x_forward(2 + k)
    for d in (0, 1):
        x_send(n_blocks - 1, d, 0).start()
    r_step(1, 0, True)
    for k in range(1, n_parts):
        for d in (0, 1):
            x_wait(2 + k, d, 1)
        results(k)
        far_out(k)
    for k in range(1, n_parts):
        r_step(1, k, True)
    turn = min(3, near + 1)

    @pl.loop(2, turn)
    def _(t):
        for k in range(n_parts):
            r_step(t, k, False)

    x_forward(n_blocks - 1)
    for d in (0, 1):
        o_send(d, 0).start()

    @pl.loop(turn, near + 1)
    def _(t):
        for k in range(n_parts):
            r_step(t, k, False)

    local[4].wait()
    for d in (0, 1):
        x_wait(n_blocks - 1, d, 1)
        o_send(d, 1).start()
    for d in (0, 1):
        for hop in (0, 1):
            o_send(d, hop).wait_recv()
    deep = obuf.shape[0] * obuf.shape[1]

    @pl.loop(0, d_model // out_wide)
    def _(n):
        cols = pl.ds(pl.multiple_of(n * out_wide, out_wide), out_wide)
        mix_out[:, cols] = jnp.dot(
            gated[...],
            obuf[:, :, cols].reshape(deep, out_wide),
            preferred_element_type=F32,
        ).astype(BF16)

    for ch in range(n_parts):
        cols = pl.ds(*parts[ch])
        value = spread_back(z, ch)
        for d in (0, 1):
            r_send(d, near, ch).wait_recv()
            value = value + acc[d, near, :, cols].astype(F32)
        exp_out[:, cols] = value.astype(BF16)

    for a in range(n_blocks):
        for d in (0, 1):
            for hop in (0, 1):
                x_send(a, d, hop).wait_send()
    for d in (0, 1):
        for h in range(far + 1):
            if h > 0:
                for ch in held(d, h):
                    z_send(d, h, ch).wait_send()
                if meta_held(d, h):
                    m_send(d, h).wait_send()
            for ch in held(d, h):
                p_send(d, h, ch).wait_send()
            if meta_held(d, h):
                pm_send(d, h).wait_send()
        for t in range(1, near + 1):
            for ch in range(n_parts):
                r_send(d, t, ch).wait_send()
        for j in range(1, skip + 1):
            g_send(d, j).wait_send()
            if j < skip or d == 1:
                gp_send(d, j).wait_send()
            for ch in range(n_parts):
                f_send(d, j, ch).wait_send()
    for ch in range(n_parts):
        swap(ch).wait_send()
    for d in (0, 1):
        for hop in (0, 1):
            o_send(d, hop).wait_send()
    halo.wait_send()


def per_device(
    n_ep,
    n_tp,
    conv_x,
    conv_c,
    conv_b,
    conv_taps,
    w_out,
    tokens_b,
    norm_gain,
    route_b,
    route_weights,
    w_gate,
    w_up,
    w_down,
):
    n_rows, d_model = tokens_b.shape
    n_conv = conv_x.shape[0]
    cap = 2 * n_rows * TOPK // n_ep
    nz = n_ep // CORES
    far = nz // 2
    near = far // 2
    skip = far - near
    units = w_gate.shape[2]
    wide = min(256, d_model)
    any_spec = pl.BlockSpec(memory_space=pl.ANY)
    vmem = pl.BlockSpec(memory_space=pltpu.VMEM)
    dma = pltpu.SemaphoreType.DMA
    slots = n_ep * cap
    return pl.pallas_call(
        functools.partial(fused, n_ep, n_tp, cap),
        out_shape=(
            jax.ShapeDtypeStruct((n_conv, d_model), BF16),
            jax.ShapeDtypeStruct((n_rows, d_model), BF16),
        ),
        in_specs=[any_spec, vmem, vmem, vmem] + [any_spec] * 7 + [vmem],
        out_specs=(vmem, vmem),
        scratch_shapes=[
            pltpu.VMEM((CORES, nz, n_rows, d_model), BF16),
            pltpu.VMEM((CORES, nz, META_ROWS, n_rows), F32),
            pltpu.VMEM((n_tp, d_model, units), BF16),
            pltpu.VMEM((n_tp, d_model, units), BF16),
            pltpu.VMEM((n_tp, units, d_model), BF16),
            pltpu.VMEM((n_tp, w_out.shape[0], d_model), BF16),
            pltpu.VMEM((slots, d_model), BF16),
            pltpu.VMEM((slots, LANES), F32),
            pltpu.VMEM((slots, n_tp * units), BF16),
            pltpu.VMEM((nz, 2 * cap, d_model), BF16),
            pltpu.VMEM((nz, cap, d_model), BF16),
            pltpu.VMEM((2, near + 1, n_rows, d_model), BF16),
            pltpu.VMEM((2, 2 * cap * (skip - 1) + cap, d_model), BF16),
            pltpu.VMEM((2, 2 * cap * (skip - 1) + cap, d_model), BF16),
            pltpu.VMEM((2, 2 * cap * (skip - 1) + cap, d_model), BF16),
            pltpu.VMEM((2, skip, cap, d_model), BF16),
            pltpu.VMEM((nz, n_rows, LANES), BF16),
            pltpu.VMEM((2, n_rows, LANES), BF16),
            pltpu.VMEM((3, n_conv, d_model), BF16),
            pltpu.VMEM((n_conv + 16, wide), F32),
            pltpu.VMEM((n_conv, d_model), BF16),
            pltpu.VMEM((16, d_model), BF16),
            pltpu.VMEM((16, d_model), BF16),
            dma((9,)),
            dma((6, 2, 2)),
            dma((6, 2, 2)),
            dma((2, near, 2)),
            dma((2, near, 2)),
            dma((2, near + 1, 2)),
            dma((2, near + 1, 2)),
            dma((2, far)),
            dma((2, far)),
            dma((2, far + 1)),
            dma((2, far + 1)),
            dma((3,)),
            dma((3,)),
            dma((2, skip, 3)),
            dma((2, skip, 3)),
            dma((2, near, 3)),
            dma((2, near, 3)),
            dma((1,)),
            dma((1,)),
            dma((2, 2)),
            dma((2, 2)),
            dma((2, skip)),
            dma((2, skip)),
            dma((2, skip)),
            dma((2, skip)),
        ],
        compiler_params=pltpu.CompilerParams(
            collective_id=0, has_side_effects=True, vmem_limit_bytes=67043328
        ),
    )(
        tokens_b,
        route_b.T,
        route_weights.T,
        norm_gain[None, :],
        w_gate,
        w_up,
        w_down,
        w_out,
        conv_x,
        conv_c,
        conv_b,
        conv_taps,
    )


def solution(mesh):
    rows = P(("grp", "ep", "tp"), None)
    return jax.shard_map(
        functools.partial(per_device, mesh.shape["ep"], mesh.shape["tp"]),
        mesh=mesh,
        in_specs=(
            rows,
            rows,
            rows,
            P(),
            P("tp", None),
            rows,
            P(),
            rows,
            rows,
            P("ep", None, "tp"),
            P("ep", None, "tp"),
            P("ep", "tp", None),
        ),
        out_specs=(rows, rows),
        check_vma=False,
    )
```

```python
import functools
import jax
import jax.numpy as jnp
from jax import lax
from jax.experimental import pallas as pl
from jax.experimental.pallas import tpu as pltpu
from jax.sharding import PartitionSpec as P

TOPK = 2
CORES = 2
LANES = 128
META_ROWS = 8
MESH = pl.DeviceIdType.MESH
BF16 = jnp.bfloat16
F32 = jnp.float32


def fused(
    n_ep,
    n_tp,
    cap,
    tokens,
    route,
    weight,
    gain,
    wg,
    wu,
    wd,
    wo,
    cx,
    cc,
    cb,
    taps,
    mix_out,
    exp_out,
    tok,
    meta_buf,
    gbuf,
    ubuf,
    dbuf,
    obuf,
    rows,
    wslot,
    hid,
    rcat,
    rout,
    acc,
    crecv,
    gsend,
    grecv,
    gother,
    pt,
    ptf,
    conv,
    uext,
    gated,
    halo_out,
    halo_in,
    lsem,
    xs,
    xr,
    zs,
    zr,
    ps,
    pr,
    ms,
    mr,
    pms,
    pmr,
    qs,
    qr,
    fs,
    fr,
    rs,
    rr,
    hs,
    hr,
    osem,
    orsem,
    gs,
    gr,
    gps,
    gpr,
):
    nz = n_ep // CORES
    far = nz // 2
    near = far // 2
    skip = far - near
    ep = lax.axis_index("ep")
    tp = lax.axis_index("tp")
    z = ep // CORES
    core = ep % CORES
    n_rows = tokens.shape[0]
    d_model = tokens.shape[1]
    half = n_rows // 2

    tp_at = [{"tp": (tp + 1) % n_tp}, {"tp": (tp + n_tp - 1) % n_tp}]
    z_at = [
        {"ep": ((z + 1) % nz) * CORES + core},
        {"ep": ((z + nz - 1) % nz) * CORES + core},
    ]
    def z_to(d, j):
        return {"ep": ((z + (j if d == 0 else nz - j)) % nz) * CORES + core}

    partner = {"ep": z * CORES + (1 - core)}
    lin = ep * n_tp + tp
    total = n_ep * n_tp
    after = (lin + 1) % total
    prior = (lin + total - 1) % total
    after_at = {"ep": after // n_tp, "tp": after % n_tp}
    prior_at = {"ep": prior // n_tp, "tp": prior % n_tp}

    barrier = pltpu.get_barrier_semaphore()
    peers = tp_at + z_at + [partner, after_at, prior_at]
    for j in range(2, skip + 1):
        peers += [z_to(0, j), z_to(1, j)]
    for peer in peers:
        pl.semaphore_signal(barrier, inc=1, device_id=peer, device_id_type=MESH)

    local = [
        pltpu.make_async_copy(tokens, tok.at[0, z], lsem.at[0]),
        pltpu.make_async_copy(wg.at[0], gbuf.at[tp], lsem.at[2]),
        pltpu.make_async_copy(wu.at[0], ubuf.at[tp], lsem.at[3]),
        pltpu.make_async_copy(wd.at[0], dbuf.at[tp], lsem.at[4]),
        pltpu.make_async_copy(wo, obuf.at[tp], lsem.at[5]),
        pltpu.make_async_copy(cx, conv.at[0], lsem.at[6]),
        pltpu.make_async_copy(cc, conv.at[1], lsem.at[7]),
        pltpu.make_async_copy(cb, conv.at[2], lsem.at[8]),
    ]
    for copy in local:
        copy.start()

    quarter = d_model // 4
    parts = [(k * quarter, quarter) for k in range(4)]
    n_parts = len(parts)
    blocks = [(wg, gbuf, None), (wu, ubuf, None)]
    blocks += [(wd, dbuf, k) for k in range(n_parts)] + [(wo, obuf, None)]
    n_blocks = len(blocks)

    def x_send(a, d, hop):
        src, buf, part = blocks[a]
        cols = () if part is None else (pl.ds(*parts[part]),)
        depth = buf.shape[1]
        base = 0
        if a == n_blocks - 1:
            depth = depth // CORES
            base = core * depth
        if hop == 0:
            every = (pl.ds(base, depth),)
            src = src.at[((0,) if src.shape[0] == 1 else ()) + every + cols]
            dst = buf.at[(tp,) + every + cols]
        else:
            owner = (tp + n_tp - 1) % n_tp if d == 0 else (tp + 1) % n_tp
            dst = buf.at[(owner, pl.ds(base + d * (depth // 2), depth // 2)) + cols]
            src = dst
        return pltpu.make_async_remote_copy(
            src_ref=src,
            dst_ref=dst,
            send_sem=xs.at[a, d, hop],
            recv_sem=xr.at[a, d, hop],
            device_id=tp_at[d],
            device_id_type=MESH,
        )

    def x_wait(a, d, hop):
        x_send(a, d, hop).wait_recv()

    def o_send(d, hop):
        depth = obuf.shape[1] // CORES
        if hop == 0:
            owner = (tp + n_tp - 1) % n_tp if d == 0 else (tp + 1) % n_tp
            at = (owner, pl.ds(core * depth, depth))
        else:
            at = ((tp + 2) % n_tp, pl.ds(core * depth + d * (depth // 2), depth // 2))
        return pltpu.make_async_remote_copy(
            src_ref=obuf.at[at],
            dst_ref=obuf.at[at],
            send_sem=osem.at[d, hop],
            recv_sem=orsem.at[d, hop],
            device_id=partner,
            device_id_type=MESH,
        )

    def x_forward(a):
        for d in (0, 1):
            x_wait(a, d, 0)
            x_send(a, d, 1).start()

    def away(d, h):
        return (z + (nz - h if d == 0 else h)) % nz

    def z_send(d, h, ch):
        ref = tok.at[0, away(d, h - 1), pl.ds(ch * half, half)]
        return pltpu.make_async_remote_copy(
            src_ref=ref,
            dst_ref=ref,
            send_sem=zs.at[d, h - 1, ch],
            recv_sem=zr.at[d, h - 1, ch],
            device_id=z_at[d],
            device_id_type=MESH,
        )

    def m_send(d, h):
        ref = meta_buf.at[0, z if h <= near else away(d, near)]
        return pltpu.make_async_remote_copy(
            src_ref=ref,
            dst_ref=ref,
            send_sem=ms.at[d, h - 1],
            recv_sem=mr.at[d, h - 1],
            device_id=z_to(d, h if h <= near else h - near),
            device_id_type=MESH,
        )

    far_rows = 2 * cap * (skip - 1) + cap

    def g_send(d, j):
        at = pl.ds((j - 1) * 2 * cap, 2 * cap if j < skip else cap)
        return pltpu.make_async_remote_copy(
            src_ref=gsend.at[d, at],
            dst_ref=grecv.at[d, at],
            send_sem=gs.at[d, j - 1],
            recv_sem=gr.at[d, j - 1],
            device_id=z_to(d, j),
            device_id_type=MESH,
        )

    def gp_send(d, j):
        base = (j - 1) * 2 * cap + (cap if j < skip else 0)
        return pltpu.make_async_remote_copy(
            src_ref=grecv.at[d, pl.ds(base, cap)],
            dst_ref=gother.at[d, j - 1],
            send_sem=gps.at[d, j - 1],
            recv_sem=gpr.at[d, j - 1],
            device_id=partner,
            device_id_type=MESH,
        )

    def p_send(d, h, ch):
        at = (away(d, h), pl.ds(ch * half, half))
        return pltpu.make_async_remote_copy(
            src_ref=tok.at[(0,) + at],
            dst_ref=tok.at[(1,) + at],
            send_sem=ps.at[d, h, ch],
            recv_sem=pr.at[d, h, ch],
            device_id=partner,
            device_id_type=MESH,
        )

    def pm_send(d, h):
        at = away(d, h)
        return pltpu.make_async_remote_copy(
            src_ref=meta_buf.at[0, at],
            dst_ref=meta_buf.at[1, at],
            send_sem=pms.at[d, h],
            recv_sem=pmr.at[d, h],
            device_id=partner,
            device_id_type=MESH,
        )

    def held(d, h):
        if h == 0:
            return (0, 1) if d == 0 else ()
        return (0, 1) if h <= near else ()

    def meta_held(d, h):
        return 0 < h < far or d == 0

    halo = pltpu.make_async_remote_copy(
        src_ref=halo_out,
        dst_ref=halo_in,
        send_sem=hs.at[0],
        recv_sem=hr.at[0],
        device_id=after_at,
        device_id_type=MESH,
    )

    tri = (
        lax.broadcasted_iota(jnp.int32, (LANES, LANES), 0)
        < lax.broadcasted_iota(jnp.int32, (LANES, LANES), 1)
    ).astype(F32).astype(BF16)

    def normalise(rel, zz, got):
        base = pl.multiple_of((rel * nz + zz) * cap, cap)
        mean = jnp.mean(got * got, axis=-1, keepdims=True)
        normed = got * lax.rsqrt(mean + 1e-06) * gain[...]
        rows[pl.ds(base, cap), :] = normed.astype(BF16)

    def select(rel, zz, dense=True):
        info = meta_buf[rel, zz]
        first, second = info[0:1], info[1:2]
        mine = ep.astype(F32)
        other = (z * CORES + (1 - core)).astype(F32)
        one = jnp.ones((1, LANES), F32)
        none = jnp.zeros((1, LANES), F32)
        hit = jnp.where(first == mine, one, jnp.where(second == mine, one, none))
        hit_p = jnp.where(first == other, one, jnp.where(second == other, one, none))
        share = jnp.where(
            first == mine, info[2:3], jnp.where(second == mine, info[3:4], none)
        )
        at_row = lax.broadcasted_iota(jnp.int32, (META_ROWS, LANES), 0)
        both = jnp.where(at_row == 0, hit, jnp.where(at_row == 1, hit_p, 0.0))
        rank = jnp.dot(both.astype(BF16), tri, preferred_element_type=F32)
        place = jnp.where(hit > 0, rank[0:1], -1.0)
        place_p = jnp.where(hit_p > 0, rank[1:2] + float(cap), -1.0)
        slot = lax.broadcasted_iota(jnp.int32, (LANES, LANES), 0).astype(F32)
        pick = jnp.where(slot[:cap] == place, 1.0, 0.0)
        base = pl.multiple_of((rel * nz + zz) * cap, cap)
        if dense:
            normalise(
                rel, zz, jnp.dot(pick.astype(BF16), tok[rel, zz], preferred_element_type=F32)
            )
        weight = jnp.sum(pick * share, axis=-1, keepdims=True)
        wslot[pl.ds(base, cap), :] = jnp.broadcast_to(weight, (cap, LANES))
        spread = jnp.where(slot == place, 1.0, jnp.where(slot == place_p, 1.0, 0.0))
        return spread

    def slot_rows(info, d, ahead):
        first, second = info[0:1], info[1:2]
        one = jnp.ones((1, LANES), F32)
        none = jnp.zeros((1, LANES), F32)
        at_row = lax.broadcasted_iota(jnp.int32, (META_ROWS, LANES), 0)
        hits = []
        for j in range(1, skip + 1):
            chip = (z + (j if (d == 0) == ahead else nz - j)) % nz
            for place, index in enumerate((core, 1 - core)):
                if j < skip or place == d:
                    expert = (chip * CORES + index).astype(F32)
                    hit = jnp.where(first == expert, one, jnp.where(second == expert, one, none))
                    hits.append((hit, (j - 1) * 2 * cap + (place * cap if j < skip else 0)))
        every = jnp.zeros((META_ROWS, LANES), F32)
        for i, (hit, _) in enumerate(hits):
            every = jnp.where(at_row == i, hit, every)
        rank = jnp.dot(every.astype(BF16), tri, preferred_element_type=F32)
        slot = lax.broadcasted_iota(jnp.int32, (LANES, LANES), 0).astype(F32)
        spread = jnp.zeros((LANES, LANES), F32)
        for i, (hit, base) in enumerate(hits):
            place = jnp.where(hit > 0, rank[i : i + 1] + float(base), -1.0)
            spread = jnp.where(slot == place, 1.0, spread)
        return spread

    def spread_far(d):
        info = meta_buf[0, (z + (near if d == 0 else nz - near)) % nz]
        ptf[d] = jnp.transpose(slot_rows(info, d, False)).astype(BF16)

    def compact(d):
        source = away(d, near)
        pick = slot_rows(meta_buf[0, source], d, True)[:far_rows]
        got = jnp.dot(pick.astype(BF16), tok[0, source], preferred_element_type=F32)
        gsend[d] = got.astype(BF16)

    def select_own(zz, dense=True):
        pt[zz] = jnp.transpose(select(0, zz, dense)).astype(BF16)

    def select_partner(zz, dense=True):
        select(1, zz, dense)

    local[5].wait()
    local[6].wait()
    tail = halo_out.shape[0]
    last = conv.shape[1] - tail
    halo_out[...] = (
        conv[0, pl.ds(last, tail), :].astype(F32) * conv[1, pl.ds(last, tail), :].astype(F32)
    ).astype(BF16)
    local[0].wait()
    at_row = lax.broadcasted_iota(jnp.int32, (META_ROWS, LANES), 0)
    first, second = weight[0:1], weight[1:2]
    sums = first + second
    info = jnp.where(at_row == 2, first / sums, jnp.where(at_row == 3, second / sums, 0.0))
    info = jnp.where(at_row == 1, route[1:2].astype(F32), info)
    meta_buf[0, z] = jnp.where(at_row == 0, route[0:1].astype(F32), info)
    pl.semaphore_wait(barrier, len(peers))

    halo.start()
    for h in range(1, near + 1):
        for d in (0, 1):
            m_send(d, h).start()
    for a in (0, 1, 2):
        for d in (0, 1):
            x_send(a, d, 0).start()
    for ch in (0, 1):
        for d in (0, 1):
            z_send(d, 1, ch).start()
    pm_send(0, 0).start()
    for ch in (0, 1):
        p_send(0, 0, ch).start()
    for d in (0, 1):
        m_send(d, near).wait_recv()
        pm_send(d, near).start()
    for j in range(1, skip + 1):
        for d in (0, 1):
            if meta_held(d, near + j):
                m_send(d, near + j).start()

    def convolve():
        local[7].wait()
        halo.wait_recv()
        n_conv = conv.shape[1]
        reach = taps.shape[0] - 1
        wide = uext.shape[1]
        edge = jnp.where(lin == 0, 0.0, 1.0)

        @pl.loop(0, d_model // wide)
        def _(n):
            cols = pl.ds(pl.multiple_of(n * wide, wide), wide)
            u = (conv[0, :, cols].astype(F32) * conv[1, :, cols].astype(F32)).astype(BF16)
            uext[pl.ds(tail, n_conv), :] = u.astype(F32)
            uext[pl.ds(0, tail), :] = halo_in[:, cols].astype(F32) * edge
            out = jnp.zeros((n_conv, wide), F32)
            for k in range(reach + 1):
                out = out + taps[pl.ds(k, 1), cols] * uext[pl.ds(tail - reach + k, n_conv), :]
            gated[:, cols] = (conv[2, :, cols].astype(F32) * out).astype(BF16)

    select_own(z)
    pm_send(0, 0).wait_recv()
    for ch in (0, 1):
        p_send(0, 0, ch).wait_recv()
    select_partner(z)

    for h in range(1, near + 1):
        for d in (0, 1):
            if h < near:
                m_send(d, h).wait_recv()
                pm_send(d, h).start()
        for ch in (0, 1):
            for d in (0, 1):
                z_send(d, h, ch).wait_recv()
                if h < near:
                    z_send(d, h + 1, ch).start()
                p_send(d, h, ch).start()
        if h == near:
            for d in (0, 1):
                compact(d)
                for j in range(skip, 0, -1):
                    g_send(d, j).start()
        if h == min(3, near):
            x_forward(0)
        if h == near:
            x_forward(1)
        if h == 1:
            convolve()

        @pl.loop(0, 2)
        def _(k):
            select_own((z + nz + jnp.where(k == 0, -h, h)) % nz)

        for d in (0, 1):
            pm_send(d, h).wait_recv()
            for ch in (0, 1):
                p_send(d, h, ch).wait_recv()

        @pl.loop(0, 2)
        def _(k):
            select_partner((z + nz + jnp.where(k == 0, -h, h)) % nz)

    for j in range(1, skip + 1):
        for d in (0, 1):
            if meta_held(d, near + j):
                m_send(d, near + j).wait_recv()
                pm_send(d, near + j).start()
    x_forward(2)
    for k in range(1, n_parts - 1):
        for d in (0, 1):
            x_send(2 + k, d, 0).start()
    for d in (0, 1):
        spread_far(d)
    for j in range(1, skip + 1):
        for d in (0, 1):
            if meta_held(d, near + j):
                pm_send(d, near + j).wait_recv()
                select_own(away(d, near + j), False)
                select_partner(away(d, near + j), False)
    for j in range(1, skip + 1):
        for d in (0, 1):
            g_send(d, j).wait_recv()
            if j < skip or d == 1:
                gp_send(d, j).start()
            if j < skip or d == 0:
                at = pl.ds((j - 1) * 2 * cap, cap)
                normalise(0, away(d, near + j), grecv[d, at, :].astype(F32))
    for j in range(1, skip + 1):
        for d in (0, 1):
            if j < skip or d == 1:
                gp_send(d, j).wait_recv()
                normalise(1, away(d, near + j), gother[d, j - 1].astype(F32))

    local[1].wait()
    local[2].wait()
    local[3].wait()

    def hidden(step):
        b = (tp + step) % n_tp
        width = gbuf.shape[2]
        gate_val = jnp.dot(rows[...], gbuf[b], preferred_element_type=F32)
        up_val = jnp.dot(rows[...], ubuf[b], preferred_element_type=F32)
        value = gate_val / (1.0 + jnp.exp(-gate_val)) * up_val
        hid[:, pl.ds(pl.multiple_of(b * width, width), width)] = value.astype(BF16)

    @pl.loop(0, n_tp - 1)
    def _(k):
        hidden(jnp.where(k == 0, 0, jnp.where(k == 1, 1, n_tp - 1)))

    for a in (0, 1):
        for d in (0, 1):
            x_wait(a, d, 1)
    hidden(2)
    mid = nz * cap
    depth = dbuf.shape[0] * dbuf.shape[1]
    out_wide = min(512, quarter)

    def down(rel, n, width):
        cols = pl.ds(pl.multiple_of(n * width, width), width)
        value = jnp.dot(
            hid[pl.ds(rel * mid, mid), :],
            dbuf[:, :, cols].reshape(depth, width),
            preferred_element_type=F32,
        )
        value = (value * wslot[pl.ds(rel * mid, mid), 0:1]).astype(BF16)
        return cols, value.reshape(nz, cap, width)

    def swap(ch):
        cols = pl.ds(*parts[ch])
        return pltpu.make_async_remote_copy(
            src_ref=rout.at[:, :, cols],
            dst_ref=rcat.at[:, pl.ds(cap, cap), cols],
            send_sem=qs.at[ch],
            recv_sem=qr.at[ch],
            device_id=partner,
            device_id_type=MESH,
        )

    def results(ch):
        low = parts[ch][0] // out_wide
        high = low + parts[ch][1] // out_wide

        @pl.loop(low, high)
        def _(n):
            cols, value = down(1, n, out_wide)
            rout[:, :, cols] = value

        swap(ch).start()

        @pl.loop(low, high)
        def _(n):
            cols, value = down(0, n, out_wide)
            rcat[:, pl.ds(0, cap), cols] = value

        swap(ch).wait_recv()

    def f_send(d, j, ch):
        zz = (z + (j + near if d == 0 else nz - j - near)) % nz
        size = 2 * cap if j < skip else cap
        cols = pl.ds(*parts[ch])
        return pltpu.make_async_remote_copy(
            src_ref=rcat.at[zz, pl.ds(0 if j < skip else d * cap, size), cols],
            dst_ref=crecv.at[d, pl.ds((j - 1) * 2 * cap, size), cols],
            send_sem=fs.at[d, j - 1, ch],
            recv_sem=fr.at[d, j - 1, ch],
            device_id=z_to(d, j),
            device_id_type=MESH,
        )

    def r_send(d, t, ch):
        cols = pl.ds(*parts[ch])
        return pltpu.make_async_remote_copy(
            src_ref=acc.at[d, t - 1, :, cols],
            dst_ref=acc.at[d, t, :, cols],
            send_sem=rs.at[d, t - 1, ch],
            recv_sem=rr.at[d, t - 1, ch],
            device_id=z_at[d],
            device_id_type=MESH,
        )

    def spread_back(zz, ch):
        return jnp.dot(
            pt[zz, :, 0 : 2 * cap],
            rcat[zz, :, pl.ds(*parts[ch])],
            preferred_element_type=F32,
        )

    def r_step(t, ch, first):
        cols = pl.ds(*parts[ch])
        for d in (0, 1):
            dist = near + 1 - t
            value = spread_back((z + (dist if d == 0 else nz - dist)) % nz, ch)
            if first:
                for j in range(1, skip + 1):
                    f_send(d, j, ch).wait_recv()
                value = value + jnp.dot(
                    ptf[d, :, 0:far_rows], crecv[d, :, cols], preferred_element_type=F32
                )
            else:
                r_send(d, t - 1, ch).wait_recv()
                value = value + acc[d, t - 1, :, cols].astype(F32)
            acc[d, t - 1, :, cols] = value.astype(BF16)
            r_send(d, t, ch).start()

    def far_out(ch):
        for j in range(skip, 0, -1):
            for d in (0, 1):
                f_send(d, j, ch).start()

    for d in (0, 1):
        x_wait(2, d, 1)
    results(0)
    far_out(0)
    last = n_parts - 1
    for k in range(1, last):
        x_forward(2 + k)
    for d in (0, 1):
        x_send(2 + last, d, 0).start()

    def part(k):
        for d in (0, 1):
            x_wait(2 + k, d, 1)
        results(k)
        far_out(k)

    for k in range(1, last):
        part(k)
    r_step(1, 0, True)
    x_forward(2 + last)
    for d in (0, 1):
        x_send(n_blocks - 1, d, 0).start()
    part(last)
    for k in range(1, n_parts):
        r_step(1, k, True)
    turn = min(3, near + 1)

    @pl.loop(2, turn)
    def _(t):
        for k in range(n_parts):
            r_step(t, k, False)

    x_forward(n_blocks - 1)
    for d in (0, 1):
        o_send(d, 0).start()

    @pl.loop(turn, near + 1)
    def _(t):
        for k in range(n_parts):
            r_step(t, k, False)

    local[4].wait()
    for d in (0, 1):
        x_wait(n_blocks - 1, d, 1)
        o_send(d, 1).start()
    for d in (0, 1):
        for hop in (0, 1):
            o_send(d, hop).wait_recv()
    deep = obuf.shape[0] * obuf.shape[1]

    @pl.loop(0, d_model // out_wide)
    def _(n):
        cols = pl.ds(pl.multiple_of(n * out_wide, out_wide), out_wide)
        mix_out[:, cols] = jnp.dot(
            gated[...],
            obuf[:, :, cols].reshape(deep, out_wide),
            preferred_element_type=F32,
        ).astype(BF16)

    for ch in range(n_parts):
        cols = pl.ds(*parts[ch])
        value = spread_back(z, ch)
        for d in (0, 1):
            r_send(d, near, ch).wait_recv()
            value = value + acc[d, near, :, cols].astype(F32)
        exp_out[:, cols] = value.astype(BF16)

    for a in range(n_blocks):
        for d in (0, 1):
            for hop in (0, 1):
                x_send(a, d, hop).wait_send()
    for d in (0, 1):
        for h in range(far + 1):
            if h > 0:
                for ch in held(d, h):
                    z_send(d, h, ch).wait_send()
                if meta_held(d, h):
                    m_send(d, h).wait_send()
            for ch in held(d, h):
                p_send(d, h, ch).wait_send()
            if meta_held(d, h):
                pm_send(d, h).wait_send()
        for t in range(1, near + 1):
            for ch in range(n_parts):
                r_send(d, t, ch).wait_send()
        for j in range(1, skip + 1):
            g_send(d, j).wait_send()
            if j < skip or d == 1:
                gp_send(d, j).wait_send()
            for ch in range(n_parts):
                f_send(d, j, ch).wait_send()
    for ch in range(n_parts):
        swap(ch).wait_send()
    for d in (0, 1):
        for hop in (0, 1):
            o_send(d, hop).wait_send()
    halo.wait_send()


def per_device(
    n_ep,
    n_tp,
    conv_x,
    conv_c,
    conv_b,
    conv_taps,
    w_out,
    tokens_b,
    norm_gain,
    route_b,
    route_weights,
    w_gate,
    w_up,
    w_down,
):
    n_rows, d_model = tokens_b.shape
    n_conv = conv_x.shape[0]
    cap = 2 * n_rows * TOPK // n_ep
    nz = n_ep // CORES
    far = nz // 2
    near = far // 2
    skip = far - near
    units = w_gate.shape[2]
    wide = min(256, d_model)
    any_spec = pl.BlockSpec(memory_space=pl.ANY)
    vmem = pl.BlockSpec(memory_space=pltpu.VMEM)
    dma = pltpu.SemaphoreType.DMA
    slots = n_ep * cap
    return pl.pallas_call(
        functools.partial(fused, n_ep, n_tp, cap),
        out_shape=(
            jax.ShapeDtypeStruct((n_conv, d_model), BF16),
            jax.ShapeDtypeStruct((n_rows, d_model), BF16),
        ),
        in_specs=[any_spec, vmem, vmem, vmem] + [any_spec] * 7 + [vmem],
        out_specs=(vmem, vmem),
        scratch_shapes=[
            pltpu.VMEM((CORES, nz, n_rows, d_model), BF16),
            pltpu.VMEM((CORES, nz, META_ROWS, n_rows), F32),
            pltpu.VMEM((n_tp, d_model, units), BF16),
            pltpu.VMEM((n_tp, d_model, units), BF16),
            pltpu.VMEM((n_tp, units, d_model), BF16),
            pltpu.VMEM((n_tp, w_out.shape[0], d_model), BF16),
            pltpu.VMEM((slots, d_model), BF16),
            pltpu.VMEM((slots, LANES), F32),
            pltpu.VMEM((slots, n_tp * units), BF16),
            pltpu.VMEM((nz, 2 * cap, d_model), BF16),
            pltpu.VMEM((nz, cap, d_model), BF16),
            pltpu.VMEM((2, near + 1, n_rows, d_model), BF16),
            pltpu.VMEM((2, 2 * cap * (skip - 1) + cap, d_model), BF16),
            pltpu.VMEM((2, 2 * cap * (skip - 1) + cap, d_model), BF16),
            pltpu.VMEM((2, 2 * cap * (skip - 1) + cap, d_model), BF16),
            pltpu.VMEM((2, skip, cap, d_model), BF16),
            pltpu.VMEM((nz, n_rows, LANES), BF16),
            pltpu.VMEM((2, n_rows, LANES), BF16),
            pltpu.VMEM((3, n_conv, d_model), BF16),
            pltpu.VMEM((n_conv + 16, wide), F32),
            pltpu.VMEM((n_conv, d_model), BF16),
            pltpu.VMEM((16, d_model), BF16),
            pltpu.VMEM((16, d_model), BF16),
            dma((9,)),
            dma((7, 2, 2)),
            dma((7, 2, 2)),
            dma((2, near, 2)),
            dma((2, near, 2)),
            dma((2, near + 1, 2)),
            dma((2, near + 1, 2)),
            dma((2, far)),
            dma((2, far)),
            dma((2, far + 1)),
            dma((2, far + 1)),
            dma((4,)),
            dma((4,)),
            dma((2, skip, 4)),
            dma((2, skip, 4)),
            dma((2, near, 4)),
            dma((2, near, 4)),
            dma((1,)),
            dma((1,)),
            dma((2, 2)),
            dma((2, 2)),
            dma((2, skip)),
            dma((2, skip)),
            dma((2, skip)),
            dma((2, skip)),
        ],
        compiler_params=pltpu.CompilerParams(
            collective_id=0, has_side_effects=True, vmem_limit_bytes=67043328
        ),
    )(
        tokens_b,
        route_b.T,
        route_weights.T,
        norm_gain[None, :],
        w_gate,
        w_up,
        w_down,
        w_out,
        conv_x,
        conv_c,
        conv_b,
        conv_taps,
    )


def solution(mesh):
    rows = P(("grp", "ep", "tp"), None)
    return jax.shard_map(
        functools.partial(per_device, mesh.shape["ep"], mesh.shape["tp"]),
        mesh=mesh,
        in_specs=(
            rows,
            rows,
            rows,
            P(),
            P("tp", None),
            rows,
            P(),
            rows,
            rows,
            P("ep", None, "tp"),
            P("ep", None, "tp"),
            P("ep", "tp", None),
        ),
        out_specs=(rows, rows),
        check_vma=False,
    )
```
